512 devices in a mesh: sp: 32 (over z, x), dp: 16 (over y, core).
Axes of the slice: x: 4, y: 8, z: 8, core: 2. Of those that a mesh axis runs over, the one named last changes fastest.
Arguments:
- query_rows: bfloat16 [16, 4096, 2048], P('dp', 'sp'), may hold values from -6 to 6
- key_rows: bfloat16 [16, 4096, 2048], P('dp', 'sp'), may hold values from -6 to 6
- value_rows: bfloat16 [16, 4096, 2048], P('dp', 'sp'), may hold values from -6 to 6
- decay_low: bfloat16 [16, 4096, 128], P('dp', 'sp'), may hold values from -5 to 5
- rate_low: bfloat16 [16, 4096, 128], P('dp', 'sp'), may hold values from -4 to 4
- decay_up: bfloat16 [128, 2048], replicated, may hold values from -0.5 to 0.5
- rate_up: bfloat16 [128, 2048], replicated, may hold values from -0.5 to 0.5
- decay_base: float32 [2048], replicated, may hold values from -12 to -2
- norm_gain: float32 [2048], replicated, may hold values from 0.1 to 1.9
- out_weight: bfloat16 [2048, 2048], P(None, 'dp'), may hold values from -0.125 to 0.125
Outputs:
- layer_out: bfloat16 [16, 4096, 2048], P('dp', 'sp')
The draws below stay inside these ranges and needn't reach their ends.
All inputs are finite; a program needn't handle non-finite values.
Results may differ from the reference program's by a relative error of at most 0.005.
Values may be sent and summed in bfloat16 or wider, within the bound.
No kernel may reach another device: no remote copies, remote signals or barrier semaphores. Data moves between devices by JAX's collectives and lax.ppermute only.
A program may use at most 128 MiB of HBM per device.

```python
import jax
import jax.numpy as jnp
from jax import lax

D = 2048
HEADS = 32
HEAD = 64
LOW = 128
TOK_DEV = 128
WIDTH = 2048
LENGTH = 4096
BATCH = 16


def draw_decay_low(key, part):
    noise = jnp.clip(jax.random.normal(jax.random.fold_in(key, 11), (BATCH, LENGTH, LOW), jnp.float32), -4.0, 4.0)
    offsets = jax.random.uniform(jax.random.fold_in(key, 12), (BATCH, LENGTH // TOK_DEV, 1), jnp.float32, minval=-1.0, maxval=1.0)
    total = noise + jnp.repeat(offsets, TOK_DEV, axis=1)
    return jnp.clip(total, -5.0, 5.0).astype(jnp.bfloat16)


def draw_decay_base(key, part):
    picks = jax.random.randint(jax.random.fold_in(key, 21), (HEADS, 1), 0, 16)
    quick = picks < 8
    slow_rate = jax.random.uniform(jax.random.fold_in(key, 22), (HEADS, HEAD), jnp.float32, minval=0.2, maxval=1.0) / LENGTH
    quick_rate = jax.random.uniform(jax.random.fold_in(key, 23), (HEADS, HEAD), jnp.float32, minval=0.01, maxval=0.033)
    chosen = jnp.where(quick, quick_rate, slow_rate)
    return jnp.clip(jnp.log(chosen) + 0.5, -12.0, -2.0).reshape(WIDTH).astype(jnp.float32)


def block_levels(key, extent, pieces, least, top_value):
    level = 1.0
    for dim, parts in pieces:
        heights = jax.random.uniform(jax.random.fold_in(jax.random.fold_in(key, 6), dim), (parts,), jnp.float32, least / len(pieces), top_value / len(pieces))
        level = level * jnp.repeat(jnp.exp(heights), extent[dim] // parts).reshape((-1,) + (1,) * (len(extent) - 1 - dim))
    return level


def gaussian(stream_key, dims, deviation, reach, cuts=(), held_as=jnp.bfloat16):
    values = deviation * jax.random.normal(stream_key, dims, jnp.float32)
    if cuts:
        values = values * block_levels(stream_key, dims, cuts, -0.22, 0.18)
    return jnp.clip(values, -reach, reach).astype(held_as)


def setup_inputs(seed: int = 0) -> dict:
    splits = jax.random.split(jax.random.key(seed), 11)
    query_rows = gaussian(splits[0], (BATCH, LENGTH, WIDTH), 1.0, 6.0, ((0, 16), (1, 32)))
    key_rows = gaussian(splits[1], (BATCH, LENGTH, WIDTH), 1.0, 6.0, ((0, 16), (1, 32)))
    value_rows = gaussian(splits[2], (BATCH, LENGTH, WIDTH), 1.0, 6.0, ((0, 16), (1, 32)))
    decay_low = draw_decay_low(jax.random.fold_in(splits[10], 71), 0)
    rate_low = gaussian(splits[4], (BATCH, LENGTH, LOW), 1.0, 4.0, ((0, 16), (1, 32)))
    decay_up = gaussian(splits[5], (LOW, WIDTH), LOW ** -0.5, 0.5)
    rate_up = gaussian(splits[6], (LOW, WIDTH), LOW ** -0.5, 0.5)
    decay_base = draw_decay_base(jax.random.fold_in(splits[10], 71), 0)
    norm_gain = jnp.clip(1.0 + 0.18 * jax.random.normal(splits[8], (WIDTH,), jnp.float32), 0.1, 1.9)
    out_weight = gaussian(splits[9], (WIDTH, D), WIDTH ** -0.5, 0.125, ((1, 16),))
    return {"query_rows": query_rows, "key_rows": key_rows, "value_rows": value_rows, "decay_low": decay_low, "rate_low": rate_low, "decay_up": decay_up, "rate_up": rate_up, "decay_base": decay_base, "norm_gain": norm_gain, "out_weight": out_weight}


HIGHEST = lax.Precision.HIGHEST

def reference(query_rows, key_rows, value_rows, decay_low, rate_low, decay_up, rate_up, decay_base, norm_gain, out_weight):
    heads = query_rows.shape[2] // HEAD

    def one_sequence(inputs):
        reads, keyed, valued, low_decay, low_rate = inputs
        positions = reads.shape[0]
        squashed = jnp.tanh(low_decay.astype(jnp.float32)).astype(jnp.bfloat16)
        decay_pre = (decay_base + jnp.dot(squashed, decay_up, preferred_element_type=jnp.float32)).astype(jnp.bfloat16)
        rate_pre = jnp.dot(low_rate, rate_up, preferred_element_type=jnp.float32).astype(jnp.bfloat16)
        log_decay = -jnp.exp(-jax.nn.softplus(-decay_pre.astype(jnp.float32)) - 0.5)
        rate = jax.nn.sigmoid(rate_pre.astype(jnp.float32))
        head_shape = (positions, heads, HEAD)
        query_heads = reads.astype(jnp.float32).reshape(head_shape)
        key_heads = keyed.astype(jnp.float32).reshape(head_shape)
        value_heads = valued.astype(jnp.float32).reshape(head_shape)
        decay_heads = jnp.exp(log_decay).reshape(head_shape)
        unit_keys = key_heads * lax.rsqrt(1.0 + lax.optimization_barrier(jnp.sum(key_heads * key_heads, axis=-1, keepdims=True)))
        erase = unit_keys * rate.reshape(head_shape)

        def advance(state, inputs_now):
            query_now, decay_now, key_now, value_now, unit_now, erase_now = inputs_now
            removed = jnp.einsum('hvk,hk->hv', state, unit_now, precision=HIGHEST)
            state = state * decay_now[:, None, :] - removed[:, :, None] * erase_now[:, None, :] + value_now[:, :, None] * key_now[:, None, :]
            return (state, jnp.einsum('hvk,hk->hv', state, query_now, precision=HIGHEST))
        initial = jnp.zeros((heads, HEAD, HEAD), jnp.float32)
        _, readout = lax.scan(advance, initial, (query_heads, decay_heads, key_heads, value_heads, unit_keys, erase))
        average = lax.optimization_barrier(jnp.mean(readout, axis=-1, keepdims=True))
        centred = readout - average
        variance = lax.optimization_barrier(jnp.mean(centred * centred, axis=-1, keepdims=True))
        normed = (centred * lax.rsqrt(variance + 1.0)).reshape(positions, heads * HEAD)
        mix = (normed * norm_gain).astype(jnp.bfloat16)
        return jnp.dot(mix, out_weight, preferred_element_type=jnp.float32).astype(jnp.bfloat16)
    return lax.map(one_sequence, (query_rows, key_rows, value_rows, decay_low, rate_low))
```

```python
import jax
import jax.numpy as jnp
from jax import lax
from jax.experimental import pallas as pl
from jax.experimental.pallas import tpu as pltpu
from jax.sharding import Mesh
from jax.sharding import PartitionSpec as P

HEAD = 64
PAIR = 2 * HEAD
DP = ("dp_0", "dp_1")
GROUP = 4
F32 = jnp.float32
BF16 = jnp.bfloat16


def dot(left, right):
    return lax.dot_general(left, right, (((1,), (0,)), ((), ())), preferred_element_type=F32)


def dot_nt(left, right):
    return lax.dot_general(left, right, (((1,), (1,)), ((), ())), preferred_element_type=F32)


def split(value):
    high = value.astype(BF16)
    low = (value - high.astype(F32)).astype(BF16)
    return high, low


def lanes(*parts):
    return jnp.concatenate(parts, axis=1)


def rows(*parts):
    return jnp.concatenate(parts, axis=0)


def half_turn(value):
    return pltpu.roll(value, HEAD, 1)


def product(left, right):
    left_high, left_low = left
    right_high, right_low = right
    return dot(lanes(left_high, left_low), rows(right_high, right_high)) + dot(left_high, right_low)


def iota(shape, dim):
    return lax.broadcasted_iota(jnp.int32, shape, dim)


def same_head():
    return (iota((PAIR, PAIR), 0) // HEAD == iota((PAIR, PAIR), 1) // HEAD).astype(F32).astype(BF16)


def inverses(matrices, length):
    row = iota((length, length), 0)
    col = iota((length, length), 1)
    apart = row ^ col
    eye = (row == col).astype(F32)
    pieces = [split(m) for m in matrices]
    solved = [eye - jnp.where(apart == 1, m, 0.0) for m in matrices]
    block = 2
    while block < length:
        here = (apart >= block) & (apart < 2 * block)
        parts = [split(s) for s in solved]
        masked = [
            (jnp.where(here, h, jnp.zeros_like(h)), jnp.where(here, l, jnp.zeros_like(l)))
            for h, l in pieces
        ]
        inner = [split(product(c, x)) for c, x in zip(masked, parts)]
        solved = [s - product(x, d) for s, x, d in zip(solved, parts, inner)]
        block *= 2
    return [split(s) for s in solved]


def local_kernel(q_ref, k_ref, v_ref, dl_ref, rl_ref, du_ref, ru_ref, base_ref, msg_ref, r_ref, o_ref):
    length = q_ref.shape[0]
    row = iota((length, length), 0)
    col = iota((length, length), 1)
    strict = row > col
    within = row >= col
    lower = within.astype(F32).astype(BF16)
    lower_twice = lanes(lower, lower)
    ones = same_head()
    ones_twice = rows(ones, ones)
    squashed = jnp.tanh(dl_ref[...].astype(F32)).astype(BF16)
    decay_pre = (base_ref[...] + dot(squashed, du_ref[...])).astype(BF16).astype(F32)
    rate_pre = dot(rl_ref[...], ru_ref[...]).astype(BF16).astype(F32)
    decays = (-0.6065306597126334) / (1.0 + jnp.exp(-decay_pre))
    rates = 0.5 + 0.5 * jnp.tanh(0.5 * rate_pre)
    first = iota((length, PAIR), 1) < HEAD
    first_two = (iota((length, 2 * PAIR), 1) & HEAD) == 0
    first_tall = iota((2 * length, PAIR), 1) < HEAD
    pairs = q_ref.shape[1] // PAIR
    stage = []
    for p in range(pairs):
        span = slice(p * PAIR, (p + 1) * PAIR)
        q = q_ref[:, span].astype(F32)
        k = k_ref[:, span].astype(F32)
        v = v_ref[:, span]
        log_decay = decays[:, span]
        squares = dot(lanes(*split(k * k)), ones_twice)
        unit = k * lax.rsqrt(1.0 + squares)
        erase = unit * rates[:, span]
        running = dot(lower_twice, rows(*split(log_decay)))
        before = running - log_decay
        centre = running[length // 2 : length // 2 + 1]
        final = running[length - 1 :]
        back = jnp.exp(centre - running)
        centre_decay = jnp.exp(centre)
        rest_decay = jnp.exp(final - centre)
        erase_from = unit * jnp.exp(before - centre)
        read_mid = q * jnp.exp(running - centre)
        key_to = k * back
        erase_to = erase * back
        left = rows(erase_from, read_mid)
        right = rows(key_to, erase_to)
        left_high, left_low = split(left)
        left_low_turned = half_turn(left - left_high.astype(F32)).astype(BF16)
        right_high, right_low = split(right)
        right_turned = half_turn(right).astype(BF16)
        nothing = jnp.zeros_like(right_high)
        v_twice = rows(v, v)
        heads = []
        for own in (first_tall, ~first_tall):
            pairings = dot_nt(
                lanes(jnp.where(own, left_high, left_low_turned), left_high),
                lanes(jnp.where(own, right_high, right_turned), jnp.where(own, right_low, nothing)),
            )
            key_pairs = jnp.where(strict, pairings[:length, :length], 0.0)
            erase_pairs = jnp.where(strict, pairings[:length, length:], 0.0)
            read_keys = jnp.where(within, pairings[length:, :length], 0.0)
            read_erase = jnp.where(within, pairings[length:, length:], 0.0)
            applied = dot(lanes(*split(rows(key_pairs, read_keys))), v_twice)
            heads.append((erase_pairs, split(read_erase), applied))
        applied = jnp.where(first_tall, heads[0][2], heads[1][2])
        stage.append(
            dict(
                heads=heads,
                sides=lanes(erase_from * centre_decay, applied[:length]),
                own_read=applied[length:],
                read_start=read_mid * centre_decay,
                key_end=key_to * rest_decay,
                erase_end=erase_to * rest_decay,
                keep=jnp.exp(final) - 1.0,
                v_twice=v_twice,
            )
        )
    solved = inverses([h[0] for s in stage for h in s["heads"]], length)
    for p in range(pairs):
        s = stage[p]
        span = slice(p * PAIR, (p + 1) * PAIR)
        sides = split(s["sides"])
        inner = jnp.where(first_two, product(solved[2 * p], sides), product(solved[2 * p + 1], sides))
        inner = split(inner)
        taken = jnp.where(
            first_two, product(s["heads"][0][1], inner), product(s["heads"][1][1], inner)
        )
        r_ref[:, span] = s["read_start"] - taken[:, :PAIR]
        o_ref[:, span] = s["own_read"] - taken[:, PAIR:]
        ended = product(split(s["erase_end"].T), inner)
        gained = dot(lanes(*split(s["key_end"].T)), s["v_twice"])
        transfer = jnp.where(row == col, s["keep"], 0.0) - ended[:, :PAIR]
        added = gained - ended[:, PAIR:]
        msg_ref[2 * p] = jnp.where(first, transfer, half_turn(added))[:HEAD].astype(BF16)
        msg_ref[2 * p + 1] = jnp.where(first, half_turn(transfer), added)[HEAD:].astype(BF16)


def scan_kernel(msg_ref, start_ref):
    first = iota((HEAD, PAIR), 1) < HEAD
    eye = (iota((HEAD, PAIR), 0) + HEAD == iota((HEAD, PAIR), 1)).astype(F32).astype(BF16)
    nothing = jnp.zeros((HEAD, PAIR), BF16)
    state = jnp.zeros((HEAD, PAIR), F32)
    chunks = msg_ref.shape[0]
    half = HEAD // 2
    for i in range(chunks):
        start_ref[i] = jnp.where(first[:half], state[:half], state[half:]).astype(BF16)
        if i + 1 < chunks:
            high, low = split(state)
            left = lanes(jnp.where(first, high, eye), jnp.where(first, low, nothing))
            here = msg_ref[i]
            here = rows(here, here)
            state = state + dot_nt(left, lanes(here, here))


def finish_kernel(start_ref, r_ref, o_ref, gain_ref, w_ref, out_ref, mix_ref):
    length = r_ref.shape[0]

    @pl.when(pl.program_id(0) == 0)
    def _():
        ones = same_head()
        ones_twice = rows(ones, ones)
        half = HEAD // 2
        first = iota((half, PAIR), 1) < HEAD
        for p in range(r_ref.shape[1] // PAIR):
            span = slice(p * PAIR, (p + 1) * PAIR)
            one = start_ref[2 * p].astype(F32)
            two = start_ref[2 * p + 1].astype(F32)
            states = rows(
                jnp.where(first, one, 0.0),
                jnp.where(first, half_turn(one), 0.0),
                jnp.where(first, 0.0, half_turn(two)),
                jnp.where(first, 0.0, two),
            ).astype(BF16)
            readout = o_ref[:, span] + dot_nt(lanes(*split(r_ref[:, span])), lanes(states, states))
            average = dot(lanes(*split(readout)), ones_twice) * (1.0 / HEAD)
            centred = readout - average
            variance = dot(lanes(*split(centred * centred)), ones_twice) * (1.0 / HEAD)
            normed = centred * lax.rsqrt(variance + 1.0)
            mix_ref[:, span] = (normed * gain_ref[:, span]).astype(BF16)

    out_ref[...] = dot(mix_ref[...], w_ref[0]).astype(BF16)


def local_chunk(q, k, v, dl, rl, du, ru, base):
    length, width = q.shape
    heads = width // HEAD
    step = GROUP * HEAD
    wide = pl.BlockSpec((length, step), lambda i: (0, i))
    low = pl.BlockSpec(dl.shape, lambda i: (0, 0))
    up = pl.BlockSpec((du.shape[0], step), lambda i: (0, i))
    return pl.pallas_call(
        local_kernel,
        grid=(width // step,),
        in_specs=[wide, wide, wide, low, low, up, up, pl.BlockSpec((1, step), lambda i: (0, i))],
        out_specs=[pl.BlockSpec((GROUP, HEAD, PAIR), lambda i: (i, 0, 0)), wide, wide],
        out_shape=[
            jax.ShapeDtypeStruct((heads, HEAD, PAIR), BF16),
            jax.ShapeDtypeStruct((length, width), F32),
            jax.ShapeDtypeStruct((length, width), F32),
        ],
        name="local_chunk",
    )(q, k, v, dl, rl, du, ru, base.reshape(1, width))


def scan_chunks(msg):
    chunks = msg.shape[0]
    return pl.pallas_call(
        scan_kernel,
        out_shape=jax.ShapeDtypeStruct((chunks, HEAD // 2, PAIR), BF16),
        name="scan_chunks",
    )(msg)


def finish(starts, r, o, gain, weight):
    length, width = r.shape
    parts, _, cols = weight.shape
    whole = lambda a: pl.BlockSpec(a.shape, lambda j: (0,) * a.ndim)
    gain = gain.reshape(1, width)
    return pl.pallas_call(
        finish_kernel,
        grid=(parts,),
        in_specs=[
            whole(starts),
            whole(r),
            whole(o),
            whole(gain),
            pl.BlockSpec((1, width, cols), lambda j: ((j % 2) * (parts // 2) + j // 2, 0, 0)),
        ],
        out_specs=pl.BlockSpec((length, cols), lambda j: (0, j)),
        out_shape=jax.ShapeDtypeStruct((length, parts * cols), BF16),
        scratch_shapes=[pltpu.VMEM((length, width), BF16)],
        name="finish",
    )(starts, r, o, gain, weight)


def per_device(
    query_rows, key_rows, value_rows, decay_low, rate_low, decay_up, rate_up, decay_base, norm_gain, out_weight
):
    columns = lax.all_gather(lax.all_gather(out_weight, "dp_0"), "dp_1")
    columns = columns.reshape(-1, *out_weight.shape)
    msg, r, o = local_chunk(
        query_rows[0], key_rows[0], value_rows[0], decay_low[0], rate_low[0], decay_up, rate_up, decay_base
    )
    here = lax.all_to_all(msg, "sp", split_axis=0, concat_axis=0, tiled=True)
    starts = scan_chunks(here)
    back = lax.all_to_all(starts, "sp", split_axis=0, concat_axis=0, tiled=True)
    return finish(back, r, o, norm_gain, columns)[None]


def solution(mesh):
    split_mesh = Mesh(mesh.devices.reshape(mesh.shape["sp"], 8, 2), ("sp", "dp_0", "dp_1"))
    placed = (
        P(DP, "sp", None),
        P(DP, "sp", None),
        P(DP, "sp", None),
        P(DP, "sp", None),
        P(DP, "sp", None),
        P(),
        P(),
        P(),
        P(),
        P(None, DP),
    )
    return jax.shard_map(
        per_device, mesh=split_mesh, in_specs=placed, out_specs=P(DP, "sp", None), check_vma=False
    )
```

```python
import jax
import jax.numpy as jnp
from jax import lax
from jax.experimental import pallas as pl
from jax.experimental.pallas import tpu as pltpu
from jax.sharding import Mesh
from jax.sharding import PartitionSpec as P

HEAD = 64
PAIR = 2 * HEAD
DP = ("dp_0", "dp_1")
GROUP = 4
F32 = jnp.float32
BF16 = jnp.bfloat16


def dot(left, right):
    return lax.dot_general(left, right, (((1,), (0,)), ((), ())), preferred_element_type=F32)


def dot_nt(left, right):
    return lax.dot_general(left, right, (((1,), (1,)), ((), ())), preferred_element_type=F32)


def split(value):
    high = value.astype(BF16)
    low = (value - high.astype(F32)).astype(BF16)
    return high, low


def lanes(*parts):
    return jnp.concatenate(parts, axis=1)


def rows(*parts):
    return jnp.concatenate(parts, axis=0)


def half_turn(value):
    return pltpu.roll(value, HEAD, 1)


def product(left, right):
    left = lanes(*left)
    right_high, right_low = right
    if right_high.shape[1] > PAIR:
        return dot(left, rows(right_high, right_high)) + dot(left, rows(right_low, right_low))
    both = lanes(right_high, right_low)
    both = dot(left, rows(both, both))
    return both[:, :PAIR] + both[:, PAIR:]


def iota(shape, dim):
    return lax.broadcasted_iota(jnp.int32, shape, dim)


def same_head():
    return (iota((PAIR, PAIR), 0) // HEAD == iota((PAIR, PAIR), 1) // HEAD).astype(F32).astype(BF16)


def inverses(matrices, length):
    row = iota((length, length), 0)
    col = iota((length, length), 1)
    apart = row ^ col
    eye = (row == col).astype(F32)
    pieces = [split(m) for m in matrices]
    solved = [eye - jnp.where(apart == 1, m, 0.0) for m in matrices]
    block = 2
    while block < length:
        here = ((apart >= block) & (apart < 2 * block)).astype(F32).astype(BF16)
        parts = [split(s) for s in solved]
        if block < 16:
            inner = [split(product((h * here, l * here), x)) for (h, l), x in zip(pieces, parts)]
            solved = [s - product(x, d) for s, x, d in zip(solved, parts, inner)]
        else:
            spans = range(0, length, 2 * block)
            odd = lambda m: rows(*(m[at + block : at + 2 * block] for at in spans))
            here = odd(here)
            gap = jnp.zeros((block, length), BF16)
            spread = lambda m: rows(*(x for i in range(len(spans)) for x in (gap, m[i * block : (i + 1) * block])))
            inner = [split(product((odd(h) * here, odd(l) * here), x)) for (h, l), x in zip(pieces, parts)]
            taken = [product((odd(h), odd(l)), (spread(dh), spread(dl))) for (h, l), (dh, dl) in zip(parts, inner)]
            solved = [
                rows(
                    *(
                        x
                        for i, at in enumerate(spans)
                        for x in (s[at : at + block], s[at + block : at + 2 * block] - t[i * block : (i + 1) * block])
                    )
                )
                for s, t in zip(solved, taken)
            ]
        block *= 2
    return [split(s) for s in solved]


def local_kernel(q_ref, k_ref, v_ref, dl_ref, rl_ref, du_ref, ru_ref, base_ref, *outs):
    msg_ref, erase_ref, inner_ref, read_ref, own_ref = outs
    length = q_ref.shape[0]
    row = iota((length, length), 0)
    col = iota((length, length), 1)
    strict = row > col
    within = row >= col
    lower = within.astype(F32).astype(BF16)
    lower_twice = lanes(lower, lower)
    ones = same_head()
    ones_twice = rows(ones, ones)
    squashed = jnp.tanh(dl_ref[...].astype(F32)).astype(BF16)
    decay_pre = (base_ref[...] + dot(squashed, du_ref[...])).astype(BF16).astype(F32)
    rate_pre = dot(rl_ref[...], ru_ref[...]).astype(BF16).astype(F32)
    decays = (-0.6065306597126334) / (1.0 + jnp.exp(-decay_pre))
    rates = 0.5 + 0.5 * jnp.tanh(0.5 * rate_pre)
    first = iota((length, PAIR), 1) < HEAD
    first_two = (iota((length, 2 * PAIR), 1) & HEAD) == 0
    first_tall = iota((2 * length, PAIR), 1) < HEAD
    pairs = q_ref.shape[1] // PAIR
    stage = []
    for p in range(pairs):
        span = slice(p * PAIR, (p + 1) * PAIR)
        q = q_ref[:, span].astype(F32)
        k = k_ref[:, span].astype(F32)
        v = v_ref[:, span]
        log_decay = decays[:, span]
        squares = dot(lanes(*split(k * k)), ones_twice)
        unit = k * lax.rsqrt(1.0 + squares)
        erase = unit * rates[:, span]
        running = dot(lower_twice, rows(*split(log_decay)))
        before = running - log_decay
        centre = running[length // 2 : length // 2 + 1]
        final = running[length - 1 :]
        back = jnp.exp(centre - running)
        centre_decay = jnp.exp(centre)
        rest_decay = jnp.exp(final - centre)
        erase_from = unit * jnp.exp(before - centre)
        read_mid = q * jnp.exp(running - centre)
        key_to = k * back
        erase_to = erase * back
        left = rows(erase_from, read_mid)
        right = rows(key_to, erase_to)
        left_high, left_low = split(left)
        left_low_turned = half_turn(left - left_high.astype(F32)).astype(BF16)
        right_high, right_low = split(right)
        right_turned = half_turn(right).astype(BF16)
        nothing = jnp.zeros_like(right_high)
        v_twice = rows(v, v)
        heads = []
        for own in (first_tall, ~first_tall):
            pairings = dot_nt(
                lanes(jnp.where(own, left_high, left_low_turned), left_high),
                lanes(jnp.where(own, right_high, right_turned), jnp.where(own, right_low, nothing)),
            )
            key_pairs = jnp.where(strict, pairings[:length, :length], 0.0)
            erase_pairs = jnp.where(strict, pairings[:length, length:], 0.0)
            read_keys = jnp.where(within, pairings[length:, :length], 0.0)
            read_erase = jnp.where(within, pairings[length:, length:], 0.0)
            applied = dot(lanes(*split(rows(key_pairs, read_keys))), v_twice)
            heads.append((erase_pairs, split(read_erase), applied))
        applied = jnp.where(first_tall, heads[0][2], heads[1][2])
        stage.append(
            dict(
                heads=heads,
                sides=lanes(erase_from * centre_decay, applied[:length]),
                own_read=applied[length:],
                read_start=read_mid * centre_decay,
                key_end=key_to * rest_decay,
                erase_end=erase_to * rest_decay,
                keep=jnp.exp(final) - 1.0,
                v_twice=v_twice,
            )
        )
    solved = inverses([h[0] for s in stage for h in s["heads"]], length)
    for p in range(pairs):
        s = stage[p]
        span = slice(p * PAIR, (p + 1) * PAIR)
        sides = split(s["sides"])
        inner = jnp.where(first_two, product(solved[2 * p], sides), product(solved[2 * p + 1], sides))
        inner = split(inner)
        for part in range(2):
            inner_ref[p, part] = inner[part]
            erase_ref[2 * p, part] = s["heads"][0][1][part]
            erase_ref[2 * p + 1, part] = s["heads"][1][1][part]
        read_ref[:, span] = s["read_start"]
        own_ref[:, span] = s["own_read"]
        ended = product(split(s["erase_end"].T), inner)
        gained = dot(lanes(*split(s["key_end"].T)), s["v_twice"])
        transfer = jnp.where(row == col, s["keep"], 0.0) - ended[:, :PAIR]
        added = gained - ended[:, PAIR:]
        msg_ref[2 * p] = jnp.where(first, transfer, half_turn(added))[:HEAD].astype(BF16)
        msg_ref[2 * p + 1] = jnp.where(first, half_turn(transfer), added)[HEAD:].astype(BF16)


def adjust_kernel(base_ref, erase_ref, inner_ref, out_ref):
    length = base_ref.shape[0]
    first = iota((length, PAIR), 1) < HEAD
    for p in range(base_ref.shape[1] // PAIR):
        span = slice(p * PAIR, (p + 1) * PAIR)
        inner = (inner_ref[p, 0], inner_ref[p, 1])
        one = product((erase_ref[2 * p, 0], erase_ref[2 * p, 1]), inner)
        two = product((erase_ref[2 * p + 1, 0], erase_ref[2 * p + 1, 1]), inner)
        out_ref[:, span] = base_ref[:, span] - jnp.where(first, one, two)


def scan_kernel(msg_ref, after_ref, start_ref):
    first = iota((HEAD, PAIR), 1) < HEAD
    eye = (iota((HEAD, PAIR), 0) + HEAD == iota((HEAD, PAIR), 1)).astype(F32).astype(BF16)
    nothing = jnp.zeros((HEAD, PAIR), BF16)
    state = jnp.zeros((HEAD, PAIR), F32)
    chunks = msg_ref.shape[0]
    half = HEAD // 2
    for i in range(chunks):
        start_ref[i] = jnp.where(first[:half], state[:half], state[half:]).astype(BF16)
        if i + 1 < chunks:
            high, low = split(state)
            left = lanes(jnp.where(first, high, eye), jnp.where(first, low, nothing))
            here = msg_ref[i]
            here = rows(here, here)
            state = state + dot_nt(left, lanes(here, here))


def finish_kernel(start_ref, r_ref, o_ref, gain_ref, w_ref, out_ref, mix_ref, here_ref, done_ref):
    copies = [pltpu.make_async_copy(w_ref.at[k], here_ref.at[k], done_ref.at[k]) for k in range(w_ref.shape[0])]
    for copy in copies:
        copy.start()
    width = r_ref.shape[1]
    ones = same_head()
    ones_twice = rows(ones, ones)
    half = HEAD // 2
    first = iota((half, PAIR), 1) < HEAD
    for p in range(width // PAIR):
        span = slice(p * PAIR, (p + 1) * PAIR)
        one = start_ref[2 * p].astype(F32)
        two = start_ref[2 * p + 1].astype(F32)
        states = rows(
            jnp.where(first, one, 0.0),
            jnp.where(first, half_turn(one), 0.0),
            jnp.where(first, 0.0, half_turn(two)),
            jnp.where(first, 0.0, two),
        ).astype(BF16)
        readout = o_ref[:, span] + dot_nt(lanes(*split(r_ref[:, span])), lanes(states, states))
        average = dot(lanes(*split(readout)), ones_twice) * (1.0 / HEAD)
        centred = readout - average
        variance = dot(lanes(*split(centred * centred)), ones_twice) * (1.0 / HEAD)
        normed = centred * lax.rsqrt(variance + 1.0)
        mix_ref[:, span] = (normed * gain_ref[:, span]).astype(BF16)

    mix = mix_ref[...]
    for k in range(0, w_ref.shape[0], 2):
        copies[k].wait()
        copies[k + 1].wait()
        out_ref[:, k * 128 : (k + 2) * 128] = dot(mix, lanes(here_ref[k], here_ref[k + 1])).astype(BF16)


FLOPS_PER_US = 500_000_000


def budget(mib, us):
    return dict(
        compiler_params=pltpu.CompilerParams(vmem_limit_bytes=mib << 20),
        cost_estimate=pl.CostEstimate(flops=int(us * FLOPS_PER_US), transcendentals=0, bytes_accessed=1 << 20),
    )


def local_chunk(q, k, v, dl, rl, du, ru, base):
    length, width = q.shape
    heads = width // HEAD
    step = GROUP * HEAD
    wide = pl.BlockSpec((length, step), lambda i: (0, i))
    low = pl.BlockSpec(dl.shape, lambda i: (0, 0))
    up = pl.BlockSpec((du.shape[0], step), lambda i: (0, i))
    bias = pl.BlockSpec((1, step), lambda i: (0, i))
    return pl.pallas_call(
        local_kernel,
        grid=(width // step,),
        in_specs=[wide, wide, wide, low, low, up, up, bias],
        out_specs=[
            pl.BlockSpec((GROUP, HEAD, PAIR), lambda i: (i, 0, 0)),
            pl.BlockSpec((GROUP, 2, length, length), lambda i: (i, 0, 0, 0)),
            pl.BlockSpec((GROUP // 2, 2, length, 2 * PAIR), lambda i: (i, 0, 0, 0)),
            wide,
            wide,
        ],
        out_shape=[
            jax.ShapeDtypeStruct((heads, HEAD, PAIR), BF16),
            jax.ShapeDtypeStruct((heads, 2, length, length), BF16),
            jax.ShapeDtypeStruct((heads // 2, 2, length, 2 * PAIR), BF16),
            jax.ShapeDtypeStruct((length, width), F32),
            jax.ShapeDtypeStruct((length, width), F32),
        ],
        name="local_chunk",
        **budget(60, 35),
    )(q, k, v, dl, rl, du, ru, base.reshape(1, width))


def adjust(start, erase, inner, half):
    length, width = start.shape
    count = 2 * GROUP
    step = count * HEAD
    wide = pl.BlockSpec((length, step), lambda i: (0, i))
    return pl.pallas_call(
        adjust_kernel,
        grid=(width // step,),
        in_specs=[
            wide,
            pl.BlockSpec((count, 2, length, length), lambda i: (i, 0, 0, 0)),
            pl.BlockSpec((count // 2, 2, length, PAIR), lambda i: (i, 0, 0, half)),
        ],
        out_specs=wide,
        out_shape=jax.ShapeDtypeStruct((length, width), F32),
        name="adjust",
        **budget(60, 3),
    )(start, erase, inner)


def scan_chunks(msg, after):
    chunks = msg.shape[0]
    return pl.pallas_call(
        scan_kernel,
        in_specs=[pl.BlockSpec(memory_space=pltpu.VMEM), pl.BlockSpec(memory_space=pltpu.HBM)],
        out_shape=jax.ShapeDtypeStruct((chunks, HEAD // 2, PAIR), BF16),
        name="scan_chunks",
        **budget(4, 6),
    )(msg, after)


def finish(starts, r, o, gain, weight):
    length, width = r.shape
    return pl.pallas_call(
        finish_kernel,
        in_specs=[pl.BlockSpec(memory_space=pltpu.VMEM)] * 4 + [pl.BlockSpec(memory_space=pltpu.HBM)],
        out_shape=jax.ShapeDtypeStruct((length, weight.shape[0] * weight.shape[2]), BF16),
        scratch_shapes=[
            pltpu.VMEM((length, width), BF16),
            pltpu.VMEM(weight.shape, BF16),
            pltpu.SemaphoreType.DMA((weight.shape[0],)),
        ],
        name="finish",
        **budget(40, 12),
    )(starts, r, o, gain.reshape(1, width), weight)


def per_device(
    query_rows, key_rows, value_rows, decay_low, rate_low, decay_up, rate_up, decay_base, norm_gain, out_weight
):
    columns = lax.all_gather(out_weight, DP)
    msg, erase, inner, read, own_read = local_chunk(
        query_rows[0], key_rows[0], value_rows[0], decay_low[0], rate_low[0], decay_up, rate_up, decay_base
    )
    here = lax.all_to_all(msg, "sp", split_axis=0, concat_axis=0, tiled=True)
    r = adjust(read, erase, inner, 0)
    starts = scan_chunks(here, r)
    back = lax.all_to_all(starts, "sp", split_axis=0, concat_axis=0, tiled=True)
    o = adjust(own_read, erase, inner, 1)
    return finish(back, r, o, norm_gain, columns)[None]


def solution(mesh):
    split_mesh = Mesh(mesh.devices.reshape(mesh.shape["sp"], 8, 2), ("sp", "dp_0", "dp_1"))
    placed = (
        P(DP, "sp", None),
        P(DP, "sp", None),
        P(DP, "sp", None),
        P(DP, "sp", None),
        P(DP, "sp", None),
        P(),
        P(),
        P(),
        P(),
        P(None, DP),
    )
    return jax.shard_map(
        per_device, mesh=split_mesh, in_specs=placed, out_specs=P(DP, "sp", None), check_vma=False
    )
```

```python
import jax
import jax.numpy as jnp
from jax import lax
from jax.experimental import pallas as pl
from jax.experimental.pallas import tpu as pltpu
from jax.sharding import Mesh
from jax.sharding import PartitionSpec as P

HEAD = 64
PAIR = 2 * HEAD
SMALL = 16
DP = ("dp_0", "dp_1")
GROUP = 4
FLOPS_PER_US = 500_000_000
F32 = jnp.float32
BF16 = jnp.bfloat16


def dot(left, right):
    return lax.dot_general(left, right, (((1,), (0,)), ((), ())), preferred_element_type=F32)


def dot_nt(left, right):
    return lax.dot_general(left, right, (((1,), (1,)), ((), ())), preferred_element_type=F32)


def split(value):
    high = value.astype(BF16)
    low = (value - high.astype(F32)).astype(BF16)
    return high, low


def lanes(*parts):
    return jnp.concatenate(parts, axis=1)


def rows(*parts):
    return jnp.concatenate(parts, axis=0)


def half_turn(value):
    return pltpu.roll(value, HEAD, 1)


def product(left, right):
    count = left[0].shape[0]
    both = dot(rows(*left), lanes(*right))
    return both[:count, :PAIR] + (both[:count, PAIR:] + both[count:, :PAIR])


def iota(shape, dim):
    return lax.broadcasted_iota(jnp.int32, shape, dim)


def same_head():
    return (iota((PAIR, PAIR), 0) // HEAD == iota((PAIR, PAIR), 1) // HEAD).astype(F32).astype(BF16)


def spread_kernel_table(table_ref, length):
    row = iota((length, length), 0)
    col = iota((length, length), 1)
    for s in range(SMALL):
        table_ref[:, s * length : (s + 1) * length] = (
            (row == (col // SMALL) * SMALL + s).astype(F32).astype(BF16)
        )


def inverses(matrices, table_ref, length):
    blocks = length // SMALL
    lane_block = iota((SMALL, length), 1) // SMALL
    packed = []
    for m in matrices:
        compact = jnp.zeros((SMALL, length), F32)
        for at in range(blocks):
            compact = jnp.where(lane_block == at, m[at * SMALL : (at + 1) * SMALL], compact)
        packed.append(compact)
    high, low = split(rows(*packed))
    tall = high.shape[0]
    left = rows(high, low)
    eye = (iota((SMALL, length), 1) % SMALL == iota((SMALL, length), 0)).astype(F32)
    solved = [eye for _ in matrices]
    for s in range(0, SMALL, 2):
        both = dot(left, table_ref[:, s * length : (s + 2) * length])
        both = both[:tall] + both[tall:]
        for step in range(2):
            if s + step + 1 == SMALL:
                break
            column = both[:, step * length : (step + 1) * length]
            solved = [
                x - column[i * SMALL : (i + 1) * SMALL] * x[s + step : s + step + 1] for i, x in enumerate(solved)
            ]
    own = [(lane_block == at).astype(F32).astype(BF16) for at in range(blocks)]
    parts = [tuple(rows(*(p * o for o in own)) for p in split(x)) for x in solved]
    pieces = [split(m) for m in matrices]
    apart = iota((length, length), 0) ^ iota((length, length), 1)
    block = SMALL
    while block < length:
        spans = range(0, length, 2 * block)
        odd = lambda m: rows(*(m[at + block : at + 2 * block] for at in spans))
        here = odd(((apart >= block) & (apart < 2 * block)).astype(F32).astype(BF16))
        gap = jnp.zeros((block, length), BF16)
        wide = lambda m: rows(*(x for i in range(len(spans)) for x in (gap, m[i * block : (i + 1) * block])))
        put = lambda m, t: rows(
            *(
                x
                for i, at in enumerate(spans)
                for x in (m[at : at + block], m[at + block : at + 2 * block] - t[i * block : (i + 1) * block])
            )
        )
        inner = [split(product((odd(h) * here, odd(l) * here), x)) for (h, l), x in zip(pieces, parts)]
        taken = [
            split(product((odd(h), odd(l)), (wide(dh), wide(dl)))) for (h, l), (dh, dl) in zip(parts, inner)
        ]
        parts = [(put(h, th), put(l, tl)) for (h, l), (th, tl) in zip(parts, taken)]
        block *= 2
    return parts


def paired_left(value, first):
    high, low = split(value)
    turned = half_turn(value - high.astype(F32)).astype(BF16)
    return lanes(jnp.where(first, high, turned), high), lanes(jnp.where(first, turned, high), high)


def paired_right(high, low):
    gap = jnp.zeros((HEAD, high.shape[1]), BF16)
    return (
        rows(high[:HEAD], high[:HEAD], low[:HEAD], gap),
        rows(high[HEAD:], high[HEAD:], gap, low[HEAD:]),
    )


def local_kernel(
    k_ref, v_ref, dl_ref, rl_ref, du_ref, ru_ref, base_ref, msg_ref, inner_ref, right_ref, scale_ref, centre_ref, table_ref
):
    length = k_ref.shape[0]

    @pl.when(pl.program_id(0) == 0)
    def _():
        spread_kernel_table(table_ref, length)

    row = iota((length, length), 0)
    col = iota((length, length), 1)
    strict = row > col
    lower = (row >= col).astype(F32).astype(BF16)
    lower_twice = lanes(lower, lower)
    ones = same_head()
    ones_twice = rows(ones, ones)
    squashed = jnp.tanh(dl_ref[...].astype(F32)).astype(BF16)
    decay_pre = (base_ref[...] + dot(squashed, du_ref[...])).astype(BF16).astype(F32)
    rate_pre = dot(rl_ref[...], ru_ref[...]).astype(BF16).astype(F32)
    decays = (-0.6065306597126334) / (1.0 + jnp.exp(-decay_pre))
    rates = 0.5 + 0.5 * jnp.tanh(0.5 * rate_pre)
    first = iota((length, PAIR), 1) < HEAD
    second_half = iota((HEAD, PAIR), 1) >= HEAD
    diagonal = iota((HEAD, PAIR), 0) == iota((HEAD, PAIR), 1)
    pairs = k_ref.shape[1] // PAIR
    stage = []
    lower_parts = []
    for p in range(pairs):
        span = slice(p * PAIR, (p + 1) * PAIR)
        k = k_ref[:, span].astype(F32)
        v = v_ref[:, span]
        v_turned = half_turn(v.astype(F32)).astype(BF16)
        log_decay = decays[:, span]
        squares = dot(lanes(*split(k * k)), ones_twice)
        unit = k * lax.rsqrt(1.0 + squares)
        erase = unit * rates[:, span]
        running = dot(lower_twice, rows(*split(log_decay)))
        before = running - log_decay
        centre = running[length // 2 : length // 2 + 1]
        final = running[length - 1 :]
        back = jnp.exp(centre - running)
        centre_decay = jnp.exp(centre)
        scale_ref[:, span] = jnp.exp(running - centre)
        centre_ref[:, span] = centre_decay
        columns = rows(jnp.exp(final - centre), jnp.exp(final) - 1.0, jnp.zeros((6, PAIR), F32)).T
        rest_decay = columns[:, :1]
        keep = columns[:, 1:2]
        erase_from = unit * jnp.exp(before - centre)
        key_to = (k * back).T
        erase_to = (erase * back).T
        right = split(lanes(key_to, erase_to))
        right_ref[p, 0], right_ref[p, 1] = right
        key_end = split(key_to * rest_decay)
        erase_end = split(erase_to * rest_decay)
        erase_start = erase_from * centre_decay
        starts = (erase_start, half_turn(erase_start))
        for h, (left, side) in enumerate(zip(paired_left(erase_from, first), paired_right(*right))):
            pairings = dot(left, side)
            key_pairs = split(jnp.where(strict, pairings[:, :length], 0.0))
            lower_parts.append(jnp.where(strict, pairings[:, length:], 0.0))
            half = slice(h * HEAD, (h + 1) * HEAD)
            value = v if h else v_turned
            applied = dot(
                rows(lanes(*key_pairs), lanes(key_end[0][half], key_end[1][half])), rows(value, value)
            )
            stage.append(
                dict(
                    sides=split(jnp.where(first, starts[h], applied[:length])),
                    gained=applied[length:],
                    erase_end=(erase_end[0][half], erase_end[1][half]),
                    keep=keep[half],
                )
            )
    solved = inverses(lower_parts, table_ref, length)
    for i, (s, m) in enumerate(zip(stage, solved)):
        inner = split(product(m, s["sides"]))
        inner_ref[i, 0], inner_ref[i, 1] = inner
        ended = product(s["erase_end"], inner)
        gained = jnp.where(second_half, s["gained"], jnp.where(diagonal, s["keep"], 0.0))
        msg_ref[i] = (gained - ended).astype(BF16)


def read_kernel(q_ref, v_ref, scale_ref, centre_ref, right_ref, inner_ref, out_ref, token_ref):
    length = q_ref.shape[0]
    token_ref[...] = jnp.zeros_like(token_ref)
    within = iota((length, length), 0) >= iota((length, length), 1)
    first = iota((length, PAIR), 1) < HEAD
    for p in range(q_ref.shape[1] // PAIR):
        span = slice(p * PAIR, (p + 1) * PAIR)
        v = v_ref[:, span]
        v_turned = half_turn(v.astype(F32)).astype(BF16)
        read_mid = q_ref[:, span].astype(F32) * scale_ref[:, span]
        read_start = read_mid * centre_ref[:, span]
        starts = (read_start, half_turn(read_start))
        sides = paired_right(right_ref[p, 0], right_ref[p, 1])
        for h, (left, side) in enumerate(zip(paired_left(read_mid, first), sides)):
            pairings = dot(left, side)
            read_keys = split(jnp.where(within, pairings[:, :length], 0.0))
            read_erase = split(jnp.where(within, pairings[:, length:], 0.0))
            value = v if h else v_turned
            applied = dot(lanes(*read_keys), rows(value, value))
            taken = product(read_erase, (inner_ref[2 * p + h, 0], inner_ref[2 * p + h, 1]))
            high, low = split(jnp.where(first, starts[h], applied) - taken)
            out_ref[2 * p + h, 0] = high
            out_ref[2 * p + h, 1] = low


def scan_kernel(msg_ref, after_ref, start_ref):
    first = iota((HEAD, PAIR), 1) < HEAD
    eye = (iota((HEAD, PAIR), 0) + HEAD == iota((HEAD, PAIR), 1)).astype(F32).astype(BF16)
    nothing = jnp.zeros((HEAD, PAIR), BF16)
    state = jnp.zeros((HEAD, PAIR), F32)
    chunks = msg_ref.shape[0]
    half = HEAD // 2
    for i in range(chunks):
        start_ref[i] = jnp.where(first[:half], state[:half], state[half:]).astype(BF16)
        if i + 1 < chunks:
            high, low = split(state)
            left = lanes(jnp.where(first, high, eye), jnp.where(first, low, nothing))
            here = msg_ref[i]
            here = rows(here, here)
            state = state + dot_nt(left, lanes(here, here))


def finish_kernel(start_ref, read_ref, gain_ref, w_ref, out_ref, mix_ref, here_ref, done_ref):
    copies = [pltpu.make_async_copy(w_ref.at[k], here_ref.at[k], done_ref.at[k]) for k in range(w_ref.shape[0])]
    for copy in copies:
        copy.start()
    length, width = mix_ref.shape
    ones = same_head()
    ones_twice = rows(ones, ones)
    half = HEAD // 2
    first = iota((half, PAIR), 1) < HEAD
    row = iota((HEAD, PAIR), 0)
    col = iota((HEAD, PAIR), 1)
    eyes = [(row + h * HEAD == col).astype(F32) for h in range(2)]
    for p in range(width // PAIR):
        span = slice(p * PAIR, (p + 1) * PAIR)
        one = start_ref[2 * p].astype(F32)
        two = start_ref[2 * p + 1].astype(F32)
        states = rows(
            jnp.where(first, one, 0.0),
            jnp.where(first, half_turn(one), 0.0),
            jnp.where(first, 0.0, half_turn(two)),
            jnp.where(first, 0.0, two),
        ).T
        right = rows(states[:HEAD], eyes[0], states[HEAD:], eyes[1]).astype(BF16)
        left = rows(*(lanes(read_ref[2 * p, part], read_ref[2 * p + 1, part]) for part in range(2)))
        readout = dot(left, right)
        readout = readout[:length] + readout[length:]
        average = dot(lanes(*split(readout)), ones_twice) * (1.0 / HEAD)
        centred = readout - average
        variance = dot(lanes(*split(centred * centred)), ones_twice) * (1.0 / HEAD)
        normed = centred * lax.rsqrt(variance + 1.0)
        mix_ref[:, span] = (normed * gain_ref[:, span]).astype(BF16)

    mix = mix_ref[...]
    for k in range(0, w_ref.shape[0], 2):
        copies[k].wait()
        copies[k + 1].wait()
        out_ref[:, k * 128 : (k + 2) * 128] = dot(mix, lanes(here_ref[k], here_ref[k + 1])).astype(BF16)


def budget(mib, us):
    return dict(
        compiler_params=pltpu.CompilerParams(vmem_limit_bytes=mib << 20),
        cost_estimate=pl.CostEstimate(flops=int(us * FLOPS_PER_US), transcendentals=0, bytes_accessed=1 << 20),
    )


def local_chunk(k, v, dl, rl, du, ru, base):
    length, width = k.shape
    heads = width // HEAD
    step = GROUP * HEAD
    wide = pl.BlockSpec((length, step), lambda i: (0, i))
    low = pl.BlockSpec(dl.shape, lambda i: (0, 0))
    up = pl.BlockSpec((du.shape[0], step), lambda i: (0, i))
    line = pl.BlockSpec((1, step), lambda i: (0, i))
    return pl.pallas_call(
        local_kernel,
        grid=(width // step,),
        in_specs=[wide, wide, low, low, up, up, line],
        out_specs=[
            pl.BlockSpec((GROUP, HEAD, PAIR), lambda i: (i, 0, 0)),
            pl.BlockSpec((GROUP, 2, length, PAIR), lambda i: (i, 0, 0, 0)),
            pl.BlockSpec((GROUP // 2, 2, PAIR, 2 * length), lambda i: (i, 0, 0, 0)),
            wide,
            line,
        ],
        out_shape=[
            jax.ShapeDtypeStruct((heads, HEAD, PAIR), BF16),
            jax.ShapeDtypeStruct((heads, 2, length, PAIR), BF16),
            jax.ShapeDtypeStruct((heads // 2, 2, PAIR, 2 * length), BF16),
            jax.ShapeDtypeStruct((length, width), F32),
            jax.ShapeDtypeStruct((1, width), F32),
        ],
        scratch_shapes=[pltpu.VMEM((length, SMALL * length), BF16)],
        name="local_chunk",
        **budget(60, 25),
    )(k, v, dl, rl, du, ru, base.reshape(1, width))


def chunk_reads(q, v, scale, centre, right, inner):
    length, width = q.shape
    heads = width // HEAD
    count = 2 * GROUP
    step = count * HEAD
    wide = pl.BlockSpec((length, step), lambda i: (0, i))
    per_head = pl.BlockSpec((count, 2, length, PAIR), lambda i: (i, 0, 0, 0))
    return pl.pallas_call(
        read_kernel,
        grid=(width // step,),
        in_specs=[
            wide,
            wide,
            wide,
            pl.BlockSpec((1, step), lambda i: (0, i)),
            pl.BlockSpec((count // 2, 2, PAIR, 2 * length), lambda i: (i, 0, 0, 0)),
            per_head,
        ],
        out_specs=[per_head, pl.BlockSpec((8, PAIR), lambda i: (0, 0))],
        out_shape=[
            jax.ShapeDtypeStruct((heads, 2, length, PAIR), BF16),
            jax.ShapeDtypeStruct((8, PAIR), F32),
        ],
        name="chunk_reads",
        **budget(60, 8),
    )(q, v, scale, centre, right, inner)


def scan_chunks(msg, after):
    chunks = msg.shape[0]
    return pl.pallas_call(
        scan_kernel,
        in_specs=[pl.BlockSpec(memory_space=pltpu.VMEM), pl.BlockSpec(memory_space=pltpu.HBM)],
        out_shape=jax.ShapeDtypeStruct((chunks, HEAD // 2, PAIR), BF16),
        name="scan_chunks",
        **budget(4, 6),
    )(msg, after)


def finish(starts, reads, gain, weight):
    length = reads.shape[2]
    width = gain.shape[0]
    return pl.pallas_call(
        finish_kernel,
        in_specs=[pl.BlockSpec(memory_space=pltpu.VMEM)] * 3 + [pl.BlockSpec(memory_space=pltpu.HBM)],
        out_shape=jax.ShapeDtypeStruct((length, weight.shape[0] * weight.shape[2]), BF16),
        scratch_shapes=[
            pltpu.VMEM((length, width), BF16),
            pltpu.VMEM(weight.shape, BF16),
            pltpu.SemaphoreType.DMA((weight.shape[0],)),
        ],
        name="finish",
        **budget(60, 12),
    )(starts, reads, gain.reshape(1, width), weight)


def per_device(
    query_rows, key_rows, value_rows, decay_low, rate_low, decay_up, rate_up, decay_base, norm_gain, out_weight
):
    columns = lax.all_gather(out_weight, DP)
    msg, inner, right, scale, centre = local_chunk(
        key_rows[0], value_rows[0], decay_low[0], rate_low[0], decay_up, rate_up, decay_base
    )
    here = lax.all_to_all(msg, "sp", split_axis=0, concat_axis=0, tiled=True)
    reads, token = chunk_reads(query_rows[0], value_rows[0], scale, centre, right, inner)
    starts = scan_chunks(here, token)
    back = lax.all_to_all(starts, "sp", split_axis=0, concat_axis=0, tiled=True)
    return finish(back, reads, norm_gain, columns)[None]


def solution(mesh):
    split_mesh = Mesh(mesh.devices.reshape(mesh.shape["sp"], 8, 2), ("sp", "dp_0", "dp_1"))
    placed = (
        P(DP, "sp", None),
        P(DP, "sp", None),
        P(DP, "sp", None),
        P(DP, "sp", None),
        P(DP, "sp", None),
        P(),
        P(),
        P(),
        P(),
        P(None, DP),
    )
    return jax.shard_map(
        per_device, mesh=split_mesh, in_specs=placed, out_specs=P(DP, "sp", None), check_vma=False
    )
```

```python
import jax
import jax.numpy as jnp
from jax import lax
from jax.experimental import pallas as pl
from jax.experimental.pallas import tpu as pltpu
from jax.sharding import Mesh
from jax.sharding import PartitionSpec as P

HEAD = 64
PAIR = 2 * HEAD
SMALL = 16
DP = ("dp_0", "dp_1")
GROUP = 16
TOGETHER = 8
ABREAST = 8
BLOCKS = 8
FLOPS_PER_US = 500_000_000
F32 = jnp.float32
BF16 = jnp.bfloat16


def dot(left, right):
    return lax.dot_general(left, right, (((1,), (0,)), ((), ())), preferred_element_type=F32)


def dot_nt(left, right):
    return lax.dot_general(left, right, (((1,), (1,)), ((), ())), preferred_element_type=F32)


def split(value):
    high = value.astype(BF16)
    low = (value - high.astype(F32)).astype(BF16)
    return high, low


def lanes(*parts):
    return jnp.concatenate(parts, axis=1)


def rows(*parts):
    return jnp.concatenate(parts, axis=0)


def half_turn(value):
    return pltpu.roll(value, HEAD, 1)


def product(left, right):
    count = left[0].shape[0]
    both = dot(rows(*left), lanes(*right))
    return both[:count, :PAIR] + (both[:count, PAIR:] + both[count:, :PAIR])


def iota(shape, dim):
    return lax.broadcasted_iota(jnp.int32, shape, dim)


def same_head():
    return (iota((PAIR, PAIR), 0) // HEAD == iota((PAIR, PAIR), 1) // HEAD).astype(F32).astype(BF16)


def spread_kernel_table(table_ref, length):
    row = iota((length, length), 0)
    col = iota((length, length), 1)
    for s in range(SMALL):
        table_ref[:, s * length : (s + 1) * length] = (
            (row == (col // SMALL) * SMALL + s).astype(F32).astype(BF16)
        )


def inverses(matrices, table_ref, length):
    blocks = length // SMALL
    lane_block = iota((SMALL, length), 1) // SMALL
    packed = []
    for m in matrices:
        compact = jnp.zeros((SMALL, length), F32)
        for at in range(blocks):
            compact = jnp.where(lane_block == at, m[at * SMALL : (at + 1) * SMALL], compact)
        packed.append(compact)
    high, low = split(rows(*packed))
    tall = high.shape[0]
    left = rows(high, low)
    eye = (iota((SMALL, length), 1) % SMALL == iota((SMALL, length), 0)).astype(F32)
    solved = [eye for _ in matrices]
    for s in range(0, SMALL, 2):
        both = dot(left, table_ref[:, s * length : (s + 2) * length])
        both = both[:tall] + both[tall:]
        for step in range(2):
            if s + step + 1 == SMALL:
                break
            column = both[:, step * length : (step + 1) * length]
            solved = [
                x - column[i * SMALL : (i + 1) * SMALL] * x[s + step : s + step + 1] for i, x in enumerate(solved)
            ]
        if s % 4:
            yield None
    own = [(lane_block == at).astype(F32).astype(BF16) for at in range(blocks)]
    parts = [tuple(rows(*(p * o for o in own)) for p in split(x)) for x in solved]
    pieces = [split(m) for m in matrices]
    apart = iota((length, length), 0) ^ iota((length, length), 1)
    block = SMALL
    while block < length:
        spans = range(0, length, 2 * block)
        odd = lambda m: rows(*(m[at + block : at + 2 * block] for at in spans))
        here = odd(((apart >= block) & (apart < 2 * block)).astype(F32).astype(BF16))
        gap = jnp.zeros((block, length), BF16)
        wide = lambda m: rows(*(x for i in range(len(spans)) for x in (gap, m[i * block : (i + 1) * block])))
        put = lambda m, t: rows(
            *(
                x
                for i, at in enumerate(spans)
                for x in (m[at : at + block], m[at + block : at + 2 * block] - t[i * block : (i + 1) * block])
            )
        )
        yield None
        inner = [split(product((odd(h) * here, odd(l) * here), x)) for (h, l), x in zip(pieces, parts)]
        yield None
        taken = [
            split(product((odd(h), odd(l)), (wide(dh), wide(dl)))) for (h, l), (dh, dl) in zip(parts, inner)
        ]
        parts = [(put(h, th), put(l, tl)) for (h, l), (th, tl) in zip(parts, taken)]
        block *= 2
    yield parts


def paired_left(value, first):
    high, low = split(value)
    turned = half_turn(value - high.astype(F32)).astype(BF16)
    return lanes(jnp.where(first, high, turned), high), lanes(jnp.where(first, turned, high), high)


def paired_right(high, low):
    gap = jnp.zeros((HEAD, high.shape[1]), BF16)
    return (
        rows(high[:HEAD], high[:HEAD], low[:HEAD], gap),
        rows(high[HEAD:], high[HEAD:], gap, low[HEAD:]),
    )


def local_kernel(
    k_ref, v_ref, dl_ref, rl_ref, du_ref, ru_ref, base_ref, msg_ref, inner_ref, right_ref, scale_ref, centre_ref, table_ref
):
    length = k_ref.shape[0]

    @pl.when(pl.program_id(0) == 0)
    def _():
        spread_kernel_table(table_ref, length)

    row = iota((length, length), 0)
    col = iota((length, length), 1)
    strict = row > col
    lower = (row >= col).astype(F32).astype(BF16)
    lower_twice = lanes(lower, lower)
    ones = same_head()
    ones_twice = rows(ones, ones)
    squashed = jnp.tanh(dl_ref[...].astype(F32)).astype(BF16)
    first = iota((length, PAIR), 1) < HEAD
    second_half = iota((HEAD, PAIR), 1) >= HEAD
    diagonal = iota((HEAD, PAIR), 0) == iota((HEAD, PAIR), 1)

    def prepare(p):
        span = slice(p * PAIR, (p + 1) * PAIR)
        decay_pre = (base_ref[:, span] + dot(squashed, du_ref[:, span])).astype(BF16).astype(F32)
        rate_pre = dot(rl_ref[...], ru_ref[:, span]).astype(BF16).astype(F32)
        yield None
        log_decay = (-0.6065306597126334) / (1.0 + jnp.exp(-decay_pre))
        rate = 0.5 + 0.5 * jnp.tanh(0.5 * rate_pre)
        k = k_ref[:, span].astype(F32)
        v = v_ref[:, span]
        v_turned = half_turn(v.astype(F32)).astype(BF16)
        squares = dot(lanes(*split(k * k)), ones_twice)
        unit = k * lax.rsqrt(1.0 + squares)
        erase = unit * rate
        running = dot(lower_twice, rows(*split(log_decay)))
        yield None
        before = running - log_decay
        centre = running[length // 2 : length // 2 + 1]
        final = running[length - 1 :]
        back = jnp.exp(centre - running)
        centre_decay = jnp.exp(centre)
        scale_ref[:, span] = jnp.exp(running - centre)
        centre_ref[:, span] = centre_decay
        columns = rows(jnp.exp(final - centre), jnp.exp(final) - 1.0, jnp.zeros((6, PAIR), F32)).T
        rest_decay = columns[:, :1]
        keep = columns[:, 1:2]
        erase_from = unit * jnp.exp(before - centre)
        key_to = (k * back).T
        erase_to = (erase * back).T
        right = split(lanes(key_to, erase_to))
        right_ref[p, 0], right_ref[p, 1] = right
        key_end = split(key_to * rest_decay)
        erase_end = split(erase_to * rest_decay)
        erase_start = erase_from * centre_decay
        starts = (erase_start, half_turn(erase_start))
        sides = zip(paired_left(erase_from, first), paired_right(*right))
        yield None
        paired = [dot(left, side) for left, side in sides]
        yield None
        made = []
        for h, pairings in enumerate(paired):
            key_pairs = split(jnp.where(strict, pairings[:, :length], 0.0))
            half = slice(h * HEAD, (h + 1) * HEAD)
            value = v if h else v_turned
            applied = dot(
                rows(lanes(*key_pairs), lanes(key_end[0][half], key_end[1][half])), rows(value, value)
            )
            made.append(
                dict(
                    head=2 * p + h,
                    lower=jnp.where(strict, pairings[:, length:], 0.0),
                    sides=split(jnp.where(first, starts[h], applied[:length])),
                    gained=applied[length:],
                    erase_end=(erase_end[0][half], erase_end[1][half]),
                    keep=keep[half],
                )
            )
        yield made

    def solve(stage):
        for solved in inverses([s["lower"] for s in stage], table_ref, length):
            yield
        inners = [split(product(m, s["sides"])) for s, m in zip(stage, solved)]
        yield
        for s, inner in zip(stage, inners):
            head = s["head"]
            inner_ref[head, 0], inner_ref[head, 1] = inner
            ended = product(s["erase_end"], inner)
            gained = jnp.where(second_half, s["gained"], jnp.where(diagonal, s["keep"], 0.0))
            msg_ref[head] = (gained - ended).astype(BF16)

    pairs = k_ref.shape[1] // PAIR
    stage = []
    for start in range(0, pairs, TOGETHER):
        for made in zip(*(prepare(p) for p in range(start, min(start + TOGETHER, pairs)))):
            pass
        stage += [head for pair in made for head in pair]
    for _ in solve(stage):
        pass


def read_kernel(q_ref, v_ref, scale_ref, centre_ref, right_ref, inner_ref, out_ref):
    length = q_ref.shape[0]
    within = iota((length, length), 0) >= iota((length, length), 1)
    first = iota((length, PAIR), 1) < HEAD
    for p in range(q_ref.shape[1] // PAIR):
        span = slice(p * PAIR, (p + 1) * PAIR)
        v = v_ref[:, span]
        v_turned = half_turn(v.astype(F32)).astype(BF16)
        read_mid = q_ref[:, span].astype(F32) * scale_ref[:, span]
        read_start = read_mid * centre_ref[:, span]
        starts = (read_start, half_turn(read_start))
        sides = paired_right(right_ref[p, 0], right_ref[p, 1])
        for h, (left, side) in enumerate(zip(paired_left(read_mid, first), sides)):
            pairings = dot(left, side)
            read_keys = split(jnp.where(within, pairings[:, :length], 0.0))
            read_erase = split(jnp.where(within, pairings[:, length:], 0.0))
            value = v if h else v_turned
            applied = dot(lanes(*read_keys), rows(value, value))
            taken = product(read_erase, (inner_ref[2 * p + h, 0], inner_ref[2 * p + h, 1]))
            high, low = split(jnp.where(first, starts[h], applied) - taken)
            out_ref[2 * p + h, 0] = high
            out_ref[2 * p + h, 1] = low


def scan_kernel(msg_ref, start_ref):
    first = iota((HEAD, PAIR), 1) < HEAD
    eye = (iota((HEAD, PAIR), 0) + HEAD == iota((HEAD, PAIR), 1)).astype(F32).astype(BF16)
    nothing = jnp.zeros((HEAD, PAIR), BF16)
    state = jnp.zeros((HEAD, PAIR), F32)
    chunks = msg_ref.shape[0]
    half = HEAD // 2
    for i in range(chunks):
        start_ref[i] = jnp.where(first[:half], state[:half], state[half:]).astype(BF16)
        if i + 1 < chunks:
            high, low = split(state)
            left = lanes(jnp.where(first, high, eye), jnp.where(first, low, nothing))
            here = msg_ref[i]
            here = rows(here, here)
            state = state + dot_nt(left, lanes(here, here))


def finish_kernel(start_ref, read_ref, gain_ref, w_ref, out_ref, mix_ref, here_ref, done_ref):
    copies = [pltpu.make_async_copy(w_ref.at[k], here_ref.at[k], done_ref.at[k]) for k in range(w_ref.shape[0])]
    for copy in copies:
        copy.start()
    length, width = mix_ref.shape
    ones = same_head()
    ones_twice = rows(ones, ones)
    half = HEAD // 2
    first = iota((half, PAIR), 1) < HEAD
    row = iota((HEAD, PAIR), 0)
    col = iota((HEAD, PAIR), 1)
    eyes = [(row + h * HEAD == col).astype(F32) for h in range(2)]
    def mixed(p):
        span = slice(p * PAIR, (p + 1) * PAIR)
        one = start_ref[2 * p].astype(F32)
        two = start_ref[2 * p + 1].astype(F32)
        states = rows(
            jnp.where(first, one, 0.0),
            jnp.where(first, half_turn(one), 0.0),
            jnp.where(first, 0.0, half_turn(two)),
            jnp.where(first, 0.0, two),
        ).T
        right = rows(states[:HEAD], eyes[0], states[HEAD:], eyes[1]).astype(BF16)
        yield
        left = rows(*(lanes(read_ref[2 * p, part], read_ref[2 * p + 1, part]) for part in range(2)))
        readout = dot(left, right)
        yield
        readout = readout[:length] + readout[length:]
        average = dot(lanes(*split(readout)), ones_twice) * (1.0 / HEAD)
        yield
        centred = readout - average
        variance = dot(lanes(*split(centred * centred)), ones_twice) * (1.0 / HEAD)
        yield
        normed = centred * lax.rsqrt(variance + 1.0)
        mix_ref[:, span] = (normed * gain_ref[:, span]).astype(BF16)
        yield

    for start in range(0, width // PAIR, ABREAST):
        for _ in zip(*(mixed(p) for p in range(start, start + ABREAST))):
            pass
    mix = mix_ref[...]
    for k in range(0, w_ref.shape[0], BLOCKS):
        for copy in copies[k : k + BLOCKS]:
            copy.wait()
        right = lanes(*(here_ref[j] for j in range(k, k + BLOCKS)))
        out_ref[:, k * 128 : (k + BLOCKS) * 128] = dot(mix, right).astype(BF16)


def budget(mib, us):
    return dict(
        compiler_params=pltpu.CompilerParams(vmem_limit_bytes=mib << 20),
        cost_estimate=pl.CostEstimate(flops=int(us * FLOPS_PER_US), transcendentals=0, bytes_accessed=1 << 20),
    )


def local_chunk(k, v, dl, rl, du, ru, base):
    length, width = k.shape
    heads = width // HEAD
    step = GROUP * HEAD
    wide = pl.BlockSpec((length, step), lambda i: (0, i))
    low = pl.BlockSpec(dl.shape, lambda i: (0, 0))
    up = pl.BlockSpec((du.shape[0], step), lambda i: (0, i))
    line = pl.BlockSpec((1, step), lambda i: (0, i))
    return pl.pallas_call(
        local_kernel,
        grid=(width // step,),
        in_specs=[wide, wide, low, low, up, up, line],
        out_specs=[
            pl.BlockSpec((GROUP, HEAD, PAIR), lambda i: (i, 0, 0)),
            pl.BlockSpec((GROUP, 2, length, PAIR), lambda i: (i, 0, 0, 0)),
            pl.BlockSpec((GROUP // 2, 2, PAIR, 2 * length), lambda i: (i, 0, 0, 0)),
            wide,
            line,
        ],
        out_shape=[
            jax.ShapeDtypeStruct((heads, HEAD, PAIR), BF16),
            jax.ShapeDtypeStruct((heads, 2, length, PAIR), BF16),
            jax.ShapeDtypeStruct((heads // 2, 2, PAIR, 2 * length), BF16),
            jax.ShapeDtypeStruct((length, width), F32),
            jax.ShapeDtypeStruct((1, width), F32),
        ],
        scratch_shapes=[pltpu.VMEM((length, SMALL * length), BF16)],
        name="local_chunk",
        **budget(60, 25),
    )(k, v, dl, rl, du, ru, base.reshape(1, width))


def chunk_reads(q, v, scale, centre, right, inner):
    length, width = q.shape
    heads = width // HEAD
    count = GROUP // 2
    step = count * HEAD
    wide = pl.BlockSpec((length, step), lambda i: (0, i))
    per_head = pl.BlockSpec((count, 2, length, PAIR), lambda i: (i, 0, 0, 0))
    return pl.pallas_call(
        read_kernel,
        grid=(width // step,),
        in_specs=[
            wide,
            wide,
            wide,
            pl.BlockSpec((1, step), lambda i: (0, i)),
            pl.BlockSpec((count // 2, 2, PAIR, 2 * length), lambda i: (i, 0, 0, 0)),
            per_head,
        ],
        out_specs=per_head,
        out_shape=jax.ShapeDtypeStruct((heads, 2, length, PAIR), BF16),
        name="chunk_reads",
        **budget(60, 8),
    )(q, v, scale, centre, right, inner)


def scan_chunks(msg):
    chunks = msg.shape[0]
    return pl.pallas_call(
        scan_kernel,
        out_shape=jax.ShapeDtypeStruct((chunks, HEAD // 2, PAIR), BF16),
        name="scan_chunks",
        **budget(4, 6),
    )(msg)


def finish(starts, reads, gain, weight):
    length = reads.shape[2]
    width = gain.shape[0]
    return pl.pallas_call(
        finish_kernel,
        in_specs=[pl.BlockSpec(memory_space=pltpu.VMEM)] * 3 + [pl.BlockSpec(memory_space=pltpu.HBM)],
        out_shape=jax.ShapeDtypeStruct((length, weight.shape[0] * weight.shape[2]), BF16),
        scratch_shapes=[
            pltpu.VMEM((length, width), BF16),
            pltpu.VMEM(weight.shape, BF16),
            pltpu.SemaphoreType.DMA((weight.shape[0],)),
        ],
        name="finish",
        **budget(60, 12),
    )(starts, reads, gain.reshape(1, width), weight)


def per_device(
    query_rows, key_rows, value_rows, decay_low, rate_low, decay_up, rate_up, decay_base, norm_gain, out_weight
):
    columns = lax.all_gather(out_weight, DP)
    msg, inner, right, scale, centre = local_chunk(
        key_rows[0], value_rows[0], decay_low[0], rate_low[0], decay_up, rate_up, decay_base
    )
    here = lax.all_to_all(msg, "sp", split_axis=0, concat_axis=0, tiled=True)
    reads = chunk_reads(query_rows[0], value_rows[0], scale, centre, right, inner)
    here, reads = lax.optimization_barrier((here, reads))
    starts = scan_chunks(here)
    back = lax.all_to_all(starts, "sp", split_axis=0, concat_axis=0, tiled=True)
    return finish(back, reads, norm_gain, columns)[None]


def solution(mesh):
    split_mesh = Mesh(mesh.devices.reshape(mesh.shape["sp"], 8, 2), ("sp", "dp_0", "dp_1"))
    placed = (
        P(DP, "sp", None),
        P(DP, "sp", None),
        P(DP, "sp", None),
        P(DP, "sp", None),
        P(DP, "sp", None),
        P(),
        P(),
        P(),
        P(),
        P(None, DP),
    )
    return jax.shard_map(
        per_device, mesh=split_mesh, in_specs=placed, out_specs=P(DP, "sp", None), check_vma=False
    )
```

```python
import jax
import jax.numpy as jnp
from jax import lax
from jax.experimental import pallas as pl
from jax.experimental.pallas import tpu as pltpu
from jax.sharding import Mesh
from jax.sharding import PartitionSpec as P

HEAD = 64
PAIR = 2 * HEAD
SMALL = 16
DP = ("dp_0", "dp_1")
GROUP = 16
TOGETHER = 8
ABREAST = 8
READS = 4
BLOCKS = 4
FLOPS_PER_US = 500_000_000
F32 = jnp.float32
BF16 = jnp.bfloat16


def dot(left, right):
    return lax.dot_general(left, right, (((1,), (0,)), ((), ())), preferred_element_type=F32)


def dot_nt(left, right):
    return lax.dot_general(left, right, (((1,), (1,)), ((), ())), preferred_element_type=F32)


def split(value):
    high = value.astype(BF16)
    low = (value - high.astype(F32)).astype(BF16)
    return high, low


def lanes(*parts):
    return jnp.concatenate(parts, axis=1)


def rows(*parts):
    return jnp.concatenate(parts, axis=0)


def half_turn(value):
    return pltpu.roll(value, HEAD, 1)


def product(left, right):
    count = left[0].shape[0]
    both = dot(rows(*left), lanes(*right))
    return both[:count, :PAIR] + (both[:count, PAIR:] + both[count:, :PAIR])


def iota(shape, dim):
    return lax.broadcasted_iota(jnp.int32, shape, dim)


def same_head():
    return (iota((PAIR, PAIR), 0) // HEAD == iota((PAIR, PAIR), 1) // HEAD).astype(F32).astype(BF16)


def spread_kernel_table(table_ref, length):
    row = iota((length, length), 0)
    col = iota((length, length), 1)
    for s in range(SMALL):
        table_ref[:, s * length : (s + 1) * length] = (
            (row == (col // SMALL) * SMALL + s).astype(F32).astype(BF16)
        )


def inverses(matrices, table_ref, length):
    blocks = length // SMALL
    lane_block = iota((SMALL, length), 1) // SMALL
    packed = []
    for m in matrices:
        compact = jnp.zeros((SMALL, length), F32)
        for at in range(blocks):
            compact = jnp.where(lane_block == at, m[at * SMALL : (at + 1) * SMALL], compact)
        packed.append(compact)
    high, low = split(rows(*packed))
    tall = high.shape[0]
    left = rows(high, low)
    eye = (iota((SMALL, length), 1) % SMALL == iota((SMALL, length), 0)).astype(F32)
    solved = [eye for _ in matrices]
    for s in range(0, SMALL, 2):
        both = dot(left, table_ref[:, s * length : (s + 2) * length])
        both = both[:tall] + both[tall:]
        for step in range(2):
            if s + step + 1 == SMALL:
                break
            column = both[:, step * length : (step + 1) * length]
            solved = [
                x - column[i * SMALL : (i + 1) * SMALL] * x[s + step : s + step + 1] for i, x in enumerate(solved)
            ]
        if s % 4:
            yield None
    own = [(lane_block == at).astype(F32).astype(BF16) for at in range(blocks)]
    parts = [tuple(rows(*(p * o for o in own)) for p in split(x)) for x in solved]
    pieces = [split(m) for m in matrices]
    apart = iota((length, length), 0) ^ iota((length, length), 1)
    block = SMALL
    while block < length:
        spans = range(0, length, 2 * block)
        odd = lambda m: rows(*(m[at + block : at + 2 * block] for at in spans))
        here = odd(((apart >= block) & (apart < 2 * block)).astype(F32).astype(BF16))
        gap = jnp.zeros((block, length), BF16)
        wide = lambda m: rows(*(x for i in range(len(spans)) for x in (gap, m[i * block : (i + 1) * block])))
        put = lambda m, t: rows(
            *(
                x
                for i, at in enumerate(spans)
                for x in (m[at : at + block], m[at + block : at + 2 * block] - t[i * block : (i + 1) * block])
            )
        )
        yield None
        inner = [split(product((odd(h) * here, odd(l) * here), x)) for (h, l), x in zip(pieces, parts)]
        yield None
        taken = [
            split(product((odd(h), odd(l)), (wide(dh), wide(dl)))) for (h, l), (dh, dl) in zip(parts, inner)
        ]
        parts = [(put(h, th), put(l, tl)) for (h, l), (th, tl) in zip(parts, taken)]
        block *= 2
    yield parts


def paired_left(value, first):
    high, low = split(value)
    turned = half_turn(value - high.astype(F32)).astype(BF16)
    return lanes(jnp.where(first, high, turned), high), lanes(jnp.where(first, turned, high), high)


def paired_right(high, low):
    gap = jnp.zeros((HEAD, high.shape[1]), BF16)
    return (
        rows(high[:HEAD], high[:HEAD], low[:HEAD], gap),
        rows(high[HEAD:], high[HEAD:], gap, low[HEAD:]),
    )


def local_kernel(
    k_ref, v_ref, dl_ref, rl_ref, du_ref, ru_ref, base_ref, msg_ref, inner_ref, right_ref, scale_ref, centre_ref, table_ref
):
    length = k_ref.shape[0]

    @pl.when(pl.program_id(0) == 0)
    def _():
        spread_kernel_table(table_ref, length)

    row = iota((length, length), 0)
    col = iota((length, length), 1)
    strict = row > col
    lower = (row >= col).astype(F32).astype(BF16)
    lower_twice = lanes(lower, lower)
    ones = same_head()
    ones_twice = rows(ones, ones)
    squashed = jnp.tanh(dl_ref[...].astype(F32)).astype(BF16)
    first = iota((length, PAIR), 1) < HEAD
    second_half = iota((HEAD, PAIR), 1) >= HEAD
    diagonal = iota((HEAD, PAIR), 0) == iota((HEAD, PAIR), 1)

    def prepare(p):
        span = slice(p * PAIR, (p + 1) * PAIR)
        decay_pre = (base_ref[:, span] + dot(squashed, du_ref[:, span])).astype(BF16).astype(F32)
        rate_pre = dot(rl_ref[...], ru_ref[:, span]).astype(BF16).astype(F32)
        yield None
        log_decay = (-0.6065306597126334) / (1.0 + jnp.exp(-decay_pre))
        rate = 0.5 + 0.5 * jnp.tanh(0.5 * rate_pre)
        k = k_ref[:, span].astype(F32)
        v = v_ref[:, span]
        v_turned = half_turn(v.astype(F32)).astype(BF16)
        squares = dot(lanes(*split(k * k)), ones_twice)
        unit = k * lax.rsqrt(1.0 + squares)
        erase = unit * rate
        running = dot(lower_twice, rows(*split(log_decay)))
        yield None
        before = running - log_decay
        centre = running[length // 2 : length // 2 + 1]
        final = running[length - 1 :]
        back = jnp.exp(centre - running)
        centre_decay = jnp.exp(centre)
        scale_ref[:, span] = jnp.exp(running - centre)
        centre_ref[:, span] = centre_decay
        columns = rows(jnp.exp(final - centre), jnp.exp(final) - 1.0, jnp.zeros((6, PAIR), F32)).T
        rest_decay = columns[:, :1]
        keep = columns[:, 1:2]
        erase_from = unit * jnp.exp(before - centre)
        key_to = (k * back).T
        erase_to = (erase * back).T
        right = split(lanes(key_to, erase_to))
        right_ref[p, 0], right_ref[p, 1] = right
        key_end = split(key_to * rest_decay)
        erase_end = split(erase_to * rest_decay)
        erase_start = erase_from * centre_decay
        starts = (erase_start, half_turn(erase_start))
        sides = zip(paired_left(erase_from, first), paired_right(*right))
        yield None
        paired = [dot(left, side) for left, side in sides]
        yield None
        made = []
        for h, pairings in enumerate(paired):
            key_pairs = split(jnp.where(strict, pairings[:, :length], 0.0))
            half = slice(h * HEAD, (h + 1) * HEAD)
            value = v if h else v_turned
            applied = dot(
                rows(lanes(*key_pairs), lanes(key_end[0][half], key_end[1][half])), rows(value, value)
            )
            made.append(
                dict(
                    head=2 * p + h,
                    lower=jnp.where(strict, pairings[:, length:], 0.0),
                    sides=split(jnp.where(first, starts[h], applied[:length])),
                    gained=applied[length:],
                    erase_end=(erase_end[0][half], erase_end[1][half]),
                    keep=keep[half],
                )
            )
        yield made

    def solve(stage):
        for solved in inverses([s["lower"] for s in stage], table_ref, length):
            yield
        inners = [split(product(m, s["sides"])) for s, m in zip(stage, solved)]
        yield
        for s, inner in zip(stage, inners):
            head = s["head"]
            inner_ref[head, 0], inner_ref[head, 1] = inner
            ended = product(s["erase_end"], inner)
            gained = jnp.where(second_half, s["gained"], jnp.where(diagonal, s["keep"], 0.0))
            msg_ref[head] = (gained - ended).astype(BF16)

    pairs = k_ref.shape[1] // PAIR
    stage = []
    for start in range(0, pairs, TOGETHER):
        for made in zip(*(prepare(p) for p in range(start, min(start + TOGETHER, pairs)))):
            pass
        stage += [head for pair in made for head in pair]
    for _ in solve(stage):
        pass


def read_kernel(q_ref, v_ref, scale_ref, centre_ref, right_ref, inner_ref, out_ref):
    length = q_ref.shape[0]
    within = iota((length, length), 0) >= iota((length, length), 1)
    first = iota((length, PAIR), 1) < HEAD

    def read(p):
        span = slice(p * PAIR, (p + 1) * PAIR)
        v = v_ref[:, span]
        v_turned = half_turn(v.astype(F32)).astype(BF16)
        read_mid = q_ref[:, span].astype(F32) * scale_ref[:, span]
        read_start = read_mid * centre_ref[:, span]
        starts = (read_start, half_turn(read_start))
        sides = paired_right(right_ref[p, 0], right_ref[p, 1])
        paired = [dot(left, side) for left, side in zip(paired_left(read_mid, first), sides)]
        yield
        parts = []
        for h, pairings in enumerate(paired):
            read_keys = split(jnp.where(within, pairings[:, :length], 0.0))
            read_erase = split(jnp.where(within, pairings[:, length:], 0.0))
            value = v if h else v_turned
            applied = dot(lanes(*read_keys), rows(value, value))
            taken = product(read_erase, (inner_ref[2 * p + h, 0], inner_ref[2 * p + h, 1]))
            parts.append((applied, taken))
        yield
        for h, (applied, taken) in enumerate(parts):
            high, low = split(jnp.where(first, starts[h], applied) - taken)
            out_ref[2 * p + h, 0] = high
            out_ref[2 * p + h, 1] = low
        yield

    pairs = q_ref.shape[1] // PAIR
    for start in range(0, pairs, READS):
        for _ in zip(*(read(p) for p in range(start, min(start + READS, pairs)))):
            pass


def scan_kernel(msg_ref, start_ref):
    first = iota((HEAD, PAIR), 1) < HEAD
    eye = (iota((HEAD, PAIR), 0) + HEAD == iota((HEAD, PAIR), 1)).astype(F32).astype(BF16)
    nothing = jnp.zeros((HEAD, PAIR), BF16)
    state = jnp.zeros((HEAD, PAIR), F32)
    chunks = msg_ref.shape[0]
    half = HEAD // 2
    for i in range(chunks):
        start_ref[i] = jnp.where(first[:half], state[:half], state[half:]).astype(BF16)
        if i + 1 < chunks:
            high, low = split(state)
            left = lanes(jnp.where(first, high, eye), jnp.where(first, low, nothing))
            here = msg_ref[i]
            here = rows(here, here)
            state = state + dot_nt(left, lanes(here, here))


def finish_kernel(start_ref, early_ref, late_ref, gain_ref, w_ref, out_ref, mix_ref, here_ref, done_ref):
    copies = [pltpu.make_async_copy(w_ref.at[k], here_ref.at[k], done_ref.at[k]) for k in range(w_ref.shape[0])]
    for copy in copies:
        copy.start()
    length, width = mix_ref.shape
    ones = same_head()
    ones_twice = rows(ones, ones)
    half = HEAD // 2
    first = iota((half, PAIR), 1) < HEAD
    row = iota((HEAD, PAIR), 0)
    col = iota((HEAD, PAIR), 1)
    eyes = [(row + h * HEAD == col).astype(F32) for h in range(2)]
    def mixed(p):
        span = slice(p * PAIR, (p + 1) * PAIR)
        one = start_ref[2 * p].astype(F32)
        two = start_ref[2 * p + 1].astype(F32)
        states = rows(
            jnp.where(first, one, 0.0),
            jnp.where(first, half_turn(one), 0.0),
            jnp.where(first, 0.0, half_turn(two)),
            jnp.where(first, 0.0, two),
        ).T
        right = rows(states[:HEAD], eyes[0], states[HEAD:], eyes[1]).astype(BF16)
        yield
        early = early_ref.shape[0] // 2
        read_ref, q = (early_ref, p) if p < early else (late_ref, p - early)
        left = rows(*(lanes(read_ref[2 * q, part], read_ref[2 * q + 1, part]) for part in range(2)))
        readout = dot(left, right)
        yield
        readout = readout[:length] + readout[length:]
        average = dot(lanes(*split(readout)), ones_twice) * (1.0 / HEAD)
        yield
        centred = readout - average
        variance = dot(lanes(*split(centred * centred)), ones_twice) * (1.0 / HEAD)
        yield
        normed = centred * lax.rsqrt(variance + 1.0)
        mix_ref[:, span] = (normed * gain_ref[:, span]).astype(BF16)
        yield

    for start in range(0, width // PAIR, ABREAST):
        for _ in zip(*(mixed(p) for p in range(start, start + ABREAST))):
            pass
    mix = mix_ref[...]
    for k in range(0, w_ref.shape[0], BLOCKS):
        for copy in copies[k : k + BLOCKS]:
            copy.wait()
        right = lanes(*(here_ref[j] for j in range(k, k + BLOCKS)))
        out_ref[:, k * 128 : (k + BLOCKS) * 128] = dot(mix, right).astype(BF16)


def budget(mib, us):
    return dict(
        compiler_params=pltpu.CompilerParams(vmem_limit_bytes=mib << 20),
        cost_estimate=pl.CostEstimate(flops=int(us * FLOPS_PER_US), transcendentals=0, bytes_accessed=1 << 20),
    )


def local_chunk(k, v, dl, rl, du, ru, base):
    length, width = k.shape
    heads = width // HEAD
    step = GROUP * HEAD
    wide = pl.BlockSpec((length, step), lambda i: (0, i))
    low = pl.BlockSpec(dl.shape, lambda i: (0, 0))
    up = pl.BlockSpec((du.shape[0], step), lambda i: (0, i))
    line = pl.BlockSpec((1, step), lambda i: (0, i))
    return pl.pallas_call(
        local_kernel,
        grid=(width // step,),
        in_specs=[wide, wide, low, low, up, up, line],
        out_specs=[
            pl.BlockSpec((GROUP, HEAD, PAIR), lambda i: (i, 0, 0)),
            pl.BlockSpec((GROUP, 2, length, PAIR), lambda i: (i, 0, 0, 0)),
            pl.BlockSpec((GROUP // 2, 2, PAIR, 2 * length), lambda i: (i, 0, 0, 0)),
            wide,
            line,
        ],
        out_shape=[
            jax.ShapeDtypeStruct((heads, HEAD, PAIR), BF16),
            jax.ShapeDtypeStruct((heads, 2, length, PAIR), BF16),
            jax.ShapeDtypeStruct((heads // 2, 2, PAIR, 2 * length), BF16),
            jax.ShapeDtypeStruct((length, width), F32),
            jax.ShapeDtypeStruct((1, width), F32),
        ],
        scratch_shapes=[pltpu.VMEM((length, SMALL * length), BF16)],
        name="local_chunk",
        **budget(60, 25),
    )(k, v, dl, rl, du, ru, base.reshape(1, width))


def chunk_reads(part, parts, q, v, scale, centre, right, inner):
    length, width = q.shape
    heads = width // HEAD // parts
    count = GROUP // 2
    step = count * HEAD
    steps = heads // count
    at = lambda i: part * steps + i
    wide = pl.BlockSpec((length, step), lambda i: (0, at(i)))
    per_head = lambda place: pl.BlockSpec((count, 2, length, PAIR), lambda i: (place(i), 0, 0, 0))
    return pl.pallas_call(
        read_kernel,
        grid=(steps,),
        in_specs=[
            wide,
            wide,
            wide,
            pl.BlockSpec((1, step), lambda i: (0, at(i))),
            pl.BlockSpec((count // 2, 2, PAIR, 2 * length), lambda i: (at(i), 0, 0, 0)),
            per_head(at),
        ],
        out_specs=per_head(lambda i: i),
        out_shape=jax.ShapeDtypeStruct((heads, 2, length, PAIR), BF16),
        name="chunk_reads",
        **budget(60, 4),
    )(q, v, scale, centre, right, inner)


def scan_chunks(msg):
    chunks = msg.shape[0]
    return pl.pallas_call(
        scan_kernel,
        out_shape=jax.ShapeDtypeStruct((chunks, HEAD // 2, PAIR), BF16),
        name="scan_chunks",
        **budget(4, 6),
    )(msg)


def finish(starts, early, late, gain, weight):
    length = early.shape[2]
    width = gain.shape[0]
    return pl.pallas_call(
        finish_kernel,
        in_specs=[pl.BlockSpec(memory_space=pltpu.VMEM)] * 4 + [pl.BlockSpec(memory_space=pltpu.HBM)],
        out_shape=jax.ShapeDtypeStruct((length, weight.shape[0] * weight.shape[2]), BF16),
        scratch_shapes=[
            pltpu.VMEM((length, width), BF16),
            pltpu.VMEM(weight.shape, BF16),
            pltpu.SemaphoreType.DMA((weight.shape[0],)),
        ],
        name="finish",
        **budget(52, 6),
    )(starts, early, late, gain.reshape(1, width), weight)


def per_device(
    query_rows, key_rows, value_rows, decay_low, rate_low, decay_up, rate_up, decay_base, norm_gain, out_weight
):
    columns = lax.all_gather(out_weight, DP)
    msg, inner, right, scale, centre = local_chunk(
        key_rows[0], value_rows[0], decay_low[0], rate_low[0], decay_up, rate_up, decay_base
    )
    reads = (query_rows[0], value_rows[0], scale, centre, right, inner)
    here = lax.all_to_all(msg, "sp", split_axis=0, concat_axis=0, tiled=True)
    early = chunk_reads(0, 2, *reads)
    here, early = lax.optimization_barrier((here, early))
    starts = scan_chunks(here)
    back = lax.all_to_all(starts, "sp", split_axis=0, concat_axis=0, tiled=True)
    late = chunk_reads(1, 2, *reads)
    return finish(back, early, late, norm_gain, columns)[None]


def solution(mesh):
    split_mesh = Mesh(mesh.devices.reshape(mesh.shape["sp"], 8, 2), ("sp", "dp_0", "dp_1"))
    placed = (
        P(DP, "sp", None),
        P(DP, "sp", None),
        P(DP, "sp", None),
        P(DP, "sp", None),
        P(DP, "sp", None),
        P(),
        P(),
        P(),
        P(),
        P(None, DP),
    )
    return jax.shard_map(
        per_device, mesh=split_mesh, in_specs=placed, out_specs=P(DP, "sp", None), check_vma=False
    )
```

```python
import jax
import jax.numpy as jnp
from jax import lax
from jax.experimental import pallas as pl
from jax.experimental.pallas import tpu as pltpu
from jax.sharding import Mesh
from jax.sharding import PartitionSpec as P

HEAD = 64
PAIR = 2 * HEAD
SMALL = 16
DP = ("dp_0", "dp_1")
GROUP = 16
TOGETHER = 8
ABREAST = 8
RUN = 8
READS = 4
BLOCKS = 4
FLOPS_PER_US = 500_000_000
F32 = jnp.float32
BF16 = jnp.bfloat16


def dot(left, right):
    return lax.dot_general(left, right, (((1,), (0,)), ((), ())), preferred_element_type=F32)


def dot_nt(left, right):
    return lax.dot_general(left, right, (((1,), (1,)), ((), ())), preferred_element_type=F32)


def split(value):
    high = value.astype(BF16)
    low = (value - high.astype(F32)).astype(BF16)
    return high, low


def lanes(*parts):
    return jnp.concatenate(parts, axis=1)


def rows(*parts):
    return jnp.concatenate(parts, axis=0)


def half_turn(value):
    return pltpu.roll(value, HEAD, 1)


def product(left, right):
    count = left[0].shape[0]
    both = dot(rows(*left), lanes(*right))
    return both[:count, :PAIR] + (both[:count, PAIR:] + both[count:, :PAIR])


def iota(shape, dim):
    return lax.broadcasted_iota(jnp.int32, shape, dim)


def same_head():
    return (iota((PAIR, PAIR), 0) // HEAD == iota((PAIR, PAIR), 1) // HEAD).astype(F32).astype(BF16)


def spread_kernel_table(table_ref, length):
    row = iota((length, length), 0)
    col = iota((length, length), 1)
    for s in range(SMALL):
        table_ref[:, s * length : (s + 1) * length] = (
            (row == (col // SMALL) * SMALL + s).astype(F32).astype(BF16)
        )


def inverses(matrices, table_ref, length):
    blocks = length // SMALL
    lane_block = iota((SMALL, length), 1) // SMALL
    packed = []
    for m in matrices:
        compact = jnp.zeros((SMALL, length), F32)
        for at in range(blocks):
            compact = jnp.where(lane_block == at, m[at * SMALL : (at + 1) * SMALL], compact)
        packed.append(compact)
    high, low = split(rows(*packed))
    tall = high.shape[0]
    left = rows(high, low)
    eye = (iota((SMALL, length), 1) % SMALL == iota((SMALL, length), 0)).astype(F32)
    solved = [eye for _ in matrices]
    for s in range(0, SMALL, 2):
        both = dot(left, table_ref[:, s * length : (s + 2) * length])
        both = both[:tall] + both[tall:]
        for step in range(2):
            if s + step + 1 == SMALL:
                break
            column = both[:, step * length : (step + 1) * length]
            solved = [
                x - column[i * SMALL : (i + 1) * SMALL] * x[s + step : s + step + 1] for i, x in enumerate(solved)
            ]
        if s % 4:
            yield None
    own = [(lane_block == at).astype(F32).astype(BF16) for at in range(blocks)]
    parts = [tuple(rows(*(p * o for o in own)) for p in split(x)) for x in solved]
    pieces = [split(m) for m in matrices]
    apart = iota((length, length), 0) ^ iota((length, length), 1)
    block = SMALL
    while block < length:
        spans = range(0, length, 2 * block)
        odd = lambda m: rows(*(m[at + block : at + 2 * block] for at in spans))
        here = odd(((apart >= block) & (apart < 2 * block)).astype(F32).astype(BF16))
        gap = jnp.zeros((block, length), BF16)
        wide = lambda m: rows(*(x for i in range(len(spans)) for x in (gap, m[i * block : (i + 1) * block])))
        put = lambda m, t: rows(
            *(
                x
                for i, at in enumerate(spans)
                for x in (m[at : at + block], m[at + block : at + 2 * block] - t[i * block : (i + 1) * block])
            )
        )
        yield None
        inner = [split(product((odd(h) * here, odd(l) * here), x)) for (h, l), x in zip(pieces, parts)]
        yield None
        taken = [
            split(product((odd(h), odd(l)), (wide(dh), wide(dl)))) for (h, l), (dh, dl) in zip(parts, inner)
        ]
        parts = [(put(h, th), put(l, tl)) for (h, l), (th, tl) in zip(parts, taken)]
        block *= 2
    yield parts


def paired_left(value, first):
    high, low = split(value)
    turned = half_turn(value - high.astype(F32)).astype(BF16)
    return lanes(jnp.where(first, high, turned), high), lanes(jnp.where(first, turned, high), high)


def paired_right(high, low):
    gap = jnp.zeros((HEAD, high.shape[1]), BF16)
    return (
        rows(high[:HEAD], high[:HEAD], low[:HEAD], gap),
        rows(high[HEAD:], high[HEAD:], gap, low[HEAD:]),
    )


def local_kernel(
    k_ref, v_ref, dl_ref, rl_ref, du_ref, ru_ref, base_ref, msg_ref, inner_ref, right_ref, scale_ref, centre_ref, table_ref
):
    length = k_ref.shape[0]

    @pl.when(pl.program_id(0) == 0)
    def _():
        spread_kernel_table(table_ref, length)

    row = iota((length, length), 0)
    col = iota((length, length), 1)
    strict = row > col
    lower = (row >= col).astype(F32).astype(BF16)
    lower_twice = lanes(lower, lower)
    ones = same_head()
    ones_twice = rows(ones, ones)
    squashed = jnp.tanh(dl_ref[...].astype(F32)).astype(BF16)
    first = iota((length, PAIR), 1) < HEAD
    second_half = iota((HEAD, PAIR), 1) >= HEAD
    diagonal = iota((HEAD, PAIR), 0) == iota((HEAD, PAIR), 1)

    def prepare(p):
        span = slice(p * PAIR, (p + 1) * PAIR)
        decay_pre = (base_ref[:, span] + dot(squashed, du_ref[:, span])).astype(BF16).astype(F32)
        rate_pre = dot(rl_ref[...], ru_ref[:, span]).astype(BF16).astype(F32)
        yield None
        log_decay = (-0.6065306597126334) / (1.0 + jnp.exp(-decay_pre))
        rate = 0.5 + 0.5 * jnp.tanh(0.5 * rate_pre)
        k = k_ref[:, span].astype(F32)
        v = v_ref[:, span]
        v_turned = half_turn(v.astype(F32)).astype(BF16)
        squares = dot(lanes(*split(k * k)), ones_twice)
        unit = k * lax.rsqrt(1.0 + squares)
        erase = unit * rate
        running = dot(lower_twice, rows(*split(log_decay)))
        yield None
        before = running - log_decay
        centre = running[length // 2 : length // 2 + 1]
        final = running[length - 1 :]
        back = jnp.exp(centre - running)
        centre_decay = jnp.exp(centre)
        scale_ref[:, span] = jnp.exp(running - centre)
        centre_ref[:, span] = centre_decay
        columns = rows(jnp.exp(final - centre), jnp.exp(final) - 1.0, jnp.zeros((6, PAIR), F32)).T
        rest_decay = columns[:, :1]
        keep = columns[:, 1:2]
        erase_from = unit * jnp.exp(before - centre)
        key_to = (k * back).T
        erase_to = (erase * back).T
        right = split(lanes(key_to, erase_to))
        right_ref[p, 0], right_ref[p, 1] = right
        key_end = split(key_to * rest_decay)
        erase_end = split(erase_to * rest_decay)
        erase_start = erase_from * centre_decay
        starts = (erase_start, half_turn(erase_start))
        sides = zip(paired_left(erase_from, first), paired_right(*right))
        yield None
        paired = [dot(left, side) for left, side in sides]
        yield None
        made = []
        for h, pairings in enumerate(paired):
            key_pairs = split(jnp.where(strict, pairings[:, :length], 0.0))
            half = slice(h * HEAD, (h + 1) * HEAD)
            value = v if h else v_turned
            applied = dot(
                rows(lanes(*key_pairs), lanes(key_end[0][half], key_end[1][half])), rows(value, value)
            )
            made.append(
                dict(
                    head=2 * p + h,
                    lower=jnp.where(strict, pairings[:, length:], 0.0),
                    sides=split(jnp.where(first, starts[h], applied[:length])),
                    gained=applied[length:],
                    erase_end=(erase_end[0][half], erase_end[1][half]),
                    keep=keep[half],
                )
            )
        yield made

    def solve(stage):
        for solved in inverses([s["lower"] for s in stage], table_ref, length):
            yield
        inners = [split(product(m, s["sides"])) for s, m in zip(stage, solved)]
        yield
        for s, inner in zip(stage, inners):
            head = s["head"]
            inner_ref[head, 0], inner_ref[head, 1] = inner
            ended = product(s["erase_end"], inner)
            gained = jnp.where(second_half, s["gained"], jnp.where(diagonal, s["keep"], 0.0))
            msg_ref[head] = (gained - ended).astype(BF16)

    pairs = k_ref.shape[1] // PAIR
    stage = []
    for start in range(0, pairs, TOGETHER):
        for made in zip(*(prepare(p) for p in range(start, min(start + TOGETHER, pairs)))):
            pass
        stage += [head for pair in made for head in pair]
    for _ in solve(stage):
        pass


def read_kernel(q_ref, v_ref, scale_ref, centre_ref, right_ref, inner_ref, out_ref):
    length = q_ref.shape[0]
    within = iota((length, length), 0) >= iota((length, length), 1)
    first = iota((length, PAIR), 1) < HEAD

    def read(p):
        span = slice(p * PAIR, (p + 1) * PAIR)
        v = v_ref[:, span]
        v_turned = half_turn(v.astype(F32)).astype(BF16)
        read_mid = q_ref[:, span].astype(F32) * scale_ref[:, span]
        read_start = read_mid * centre_ref[:, span]
        starts = (read_start, half_turn(read_start))
        sides = paired_right(right_ref[p, 0], right_ref[p, 1])
        paired = [dot(left, side) for left, side in zip(paired_left(read_mid, first), sides)]
        yield
        parts = []
        for h, pairings in enumerate(paired):
            read_keys = split(jnp.where(within, pairings[:, :length], 0.0))
            read_erase = split(jnp.where(within, pairings[:, length:], 0.0))
            value = v if h else v_turned
            applied = dot(lanes(*read_keys), rows(value, value))
            taken = product(read_erase, (inner_ref[2 * p + h, 0], inner_ref[2 * p + h, 1]))
            parts.append((applied, taken))
        yield
        for h, (applied, taken) in enumerate(parts):
            high, low = split(jnp.where(first, starts[h], applied) - taken)
            out_ref[2 * p + h, 0] = high
            out_ref[2 * p + h, 1] = low
        yield

    pairs = q_ref.shape[1] // PAIR
    for start in range(0, pairs, READS):
        for _ in zip(*(read(p) for p in range(start, min(start + READS, pairs)))):
            pass


def scan_kernel(msg_ref, start_ref):
    chunks = msg_ref.shape[0]
    runs = chunks // RUN
    half = HEAD // 2
    first = iota((PAIR, PAIR), 1) < HEAD
    eye = (iota((PAIR, PAIR), 0) + HEAD == iota((PAIR, PAIR), 1)).astype(F32).astype(BF16)
    nothing = jnp.zeros((PAIR, PAIR), BF16)
    begin = (iota((PAIR, PAIR), 0) == HEAD + (iota((PAIR, PAIR), 1) % HEAD)).astype(F32)

    def put(i, state):
        start_ref[i] = jnp.where(first[:half], state[:half], state[half:]).astype(BF16)

    held = [[begin if r else begin[:HEAD]] for r in range(runs)]
    parts = [[split(h[0])] for h in held]
    for j in range(RUN):
        for r in range(runs):
            if j + 1 == RUN and r + 1 == runs:
                continue
            high, low = parts[r][j]
            tall = high.shape[0]
            left = lanes(jnp.where(first[:tall], high, eye[:tall]), jnp.where(first[:tall], low, nothing[:tall]))
            here = msg_ref[r * RUN + j]
            here = rows(here, here)
            held[r].append(held[r][j] + dot_nt(left, lanes(here, here)))
            parts[r].append(split(held[r][j + 1]))
    for j in range(RUN):
        put(j, held[0][j])
    state = held[0][RUN]
    for r in range(1, runs):
        put(r * RUN, state)
        high, low = split(state)
        blank = nothing[:HEAD]
        left = lanes(jnp.where(first[:HEAD], high, low), jnp.where(first[:HEAD], high, blank))
        for j in range(RUN, 0, -1):
            if j == RUN and r + 1 == runs:
                continue
            high, low = (x[HEAD:] for x in parts[r][j])
            moved = held[r][j][:HEAD] + dot(left, rows(high, high, low, blank))
            if j == RUN:
                state = moved
            else:
                put(r * RUN + j, moved)


def finish_kernel(start_ref, early_ref, late_ref, gain_ref, w_ref, out_ref, mix_ref, here_ref, done_ref):
    copies = [pltpu.make_async_copy(w_ref.at[k], here_ref.at[k], done_ref.at[k]) for k in range(w_ref.shape[0])]
    for copy in copies:
        copy.start()
    length, width = mix_ref.shape
    ones = same_head()
    ones_twice = rows(ones, ones)
    half = HEAD // 2
    first = iota((half, PAIR), 1) < HEAD
    row = iota((HEAD, PAIR), 0)
    col = iota((HEAD, PAIR), 1)
    eyes = [(row + h * HEAD == col).astype(F32) for h in range(2)]
    def mixed(p):
        span = slice(p * PAIR, (p + 1) * PAIR)
        one = start_ref[2 * p].astype(F32)
        two = start_ref[2 * p + 1].astype(F32)
        states = rows(
            jnp.where(first, one, 0.0),
            jnp.where(first, half_turn(one), 0.0),
            jnp.where(first, 0.0, half_turn(two)),
            jnp.where(first, 0.0, two),
        ).T
        right = rows(states[:HEAD], eyes[0], states[HEAD:], eyes[1]).astype(BF16)
        yield
        early = early_ref.shape[0] // 2
        read_ref, q = (early_ref, p) if p < early else (late_ref, p - early)
        left = rows(*(lanes(read_ref[2 * q, part], read_ref[2 * q + 1, part]) for part in range(2)))
        readout = dot(left, right)
        yield
        readout = readout[:length] + readout[length:]
        average = dot(lanes(*split(readout)), ones_twice) * (1.0 / HEAD)
        yield
        centred = readout - average
        variance = dot(lanes(*split(centred * centred)), ones_twice) * (1.0 / HEAD)
        yield
        normed = centred * lax.rsqrt(variance + 1.0)
        mix_ref[:, span] = (normed * gain_ref[:, span]).astype(BF16)
        yield

    for start in range(0, width // PAIR, ABREAST):
        for _ in zip(*(mixed(p) for p in range(start, start + ABREAST))):
            pass
    mix = mix_ref[...]
    for k in range(0, w_ref.shape[0], BLOCKS):
        for copy in copies[k : k + BLOCKS]:
            copy.wait()
        right = lanes(*(here_ref[j] for j in range(k, k + BLOCKS)))
        out_ref[:, k * 128 : (k + BLOCKS) * 128] = dot(mix, right).astype(BF16)


def budget(mib, us):
    return dict(
        compiler_params=pltpu.CompilerParams(vmem_limit_bytes=mib << 20),
        cost_estimate=pl.CostEstimate(flops=int(us * FLOPS_PER_US), transcendentals=0, bytes_accessed=1 << 20),
    )


def local_chunk(k, v, dl, rl, du, ru, base):
    length, width = k.shape
    heads = width // HEAD
    step = GROUP * HEAD
    wide = pl.BlockSpec((length, step), lambda i: (0, i))
    low = pl.BlockSpec(dl.shape, lambda i: (0, 0))
    up = pl.BlockSpec((du.shape[0], step), lambda i: (0, i))
    line = pl.BlockSpec((1, step), lambda i: (0, i))
    return pl.pallas_call(
        local_kernel,
        grid=(width // step,),
        in_specs=[wide, wide, low, low, up, up, line],
        out_specs=[
            pl.BlockSpec((GROUP, HEAD, PAIR), lambda i: (i, 0, 0)),
            pl.BlockSpec((GROUP, 2, length, PAIR), lambda i: (i, 0, 0, 0)),
            pl.BlockSpec((GROUP // 2, 2, PAIR, 2 * length), lambda i: (i, 0, 0, 0)),
            wide,
            line,
        ],
        out_shape=[
            jax.ShapeDtypeStruct((heads, HEAD, PAIR), BF16),
            jax.ShapeDtypeStruct((heads, 2, length, PAIR), BF16),
            jax.ShapeDtypeStruct((heads // 2, 2, PAIR, 2 * length), BF16),
            jax.ShapeDtypeStruct((length, width), F32),
            jax.ShapeDtypeStruct((1, width), F32),
        ],
        scratch_shapes=[pltpu.VMEM((length, SMALL * length), BF16)],
        name="local_chunk",
        **budget(60, 25),
    )(k, v, dl, rl, du, ru, base.reshape(1, width))


def chunk_reads(part, parts, q, v, scale, centre, right, inner):
    length, width = q.shape
    heads = width // HEAD // parts
    count = GROUP // 2
    step = count * HEAD
    steps = heads // count
    at = lambda i: part * steps + i
    wide = pl.BlockSpec((length, step), lambda i: (0, at(i)))
    per_head = lambda place: pl.BlockSpec((count, 2, length, PAIR), lambda i: (place(i), 0, 0, 0))
    return pl.pallas_call(
        read_kernel,
        grid=(steps,),
        in_specs=[
            wide,
            wide,
            wide,
            pl.BlockSpec((1, step), lambda i: (0, at(i))),
            pl.BlockSpec((count // 2, 2, PAIR, 2 * length), lambda i: (at(i), 0, 0, 0)),
            per_head(at),
        ],
        out_specs=per_head(lambda i: i),
        out_shape=jax.ShapeDtypeStruct((heads, 2, length, PAIR), BF16),
        name="chunk_reads",
        **budget(60, 4),
    )(q, v, scale, centre, right, inner)


def scan_chunks(msg):
    chunks = msg.shape[0]
    return pl.pallas_call(
        scan_kernel,
        out_shape=jax.ShapeDtypeStruct((chunks, HEAD // 2, PAIR), BF16),
        name="scan_chunks",
        **budget(4, 6),
    )(msg)


def finish(starts, early, late, gain, weight):
    length = early.shape[2]
    width = gain.shape[0]
    return pl.pallas_call(
        finish_kernel,
        in_specs=[pl.BlockSpec(memory_space=pltpu.VMEM)] * 4 + [pl.BlockSpec(memory_space=pltpu.HBM)],
        out_shape=jax.ShapeDtypeStruct((length, weight.shape[0] * weight.shape[2]), BF16),
        scratch_shapes=[
            pltpu.VMEM((length, width), BF16),
            pltpu.VMEM(weight.shape, BF16),
            pltpu.SemaphoreType.DMA((weight.shape[0],)),
        ],
        name="finish",
        **budget(52, 6),
    )(starts, early, late, gain.reshape(1, width), weight)


def per_device(
    query_rows, key_rows, value_rows, decay_low, rate_low, decay_up, rate_up, decay_base, norm_gain, out_weight
):
    columns = lax.all_gather(out_weight, DP)
    msg, inner, right, scale, centre = local_chunk(
        key_rows[0], value_rows[0], decay_low[0], rate_low[0], decay_up, rate_up, decay_base
    )
    reads = (query_rows[0], value_rows[0], scale, centre, right, inner)
    here = lax.all_to_all(msg, "sp", split_axis=0, concat_axis=0, tiled=True)
    early = chunk_reads(0, 2, *reads)
    here, early = lax.optimization_barrier((here, early))
    starts = scan_chunks(here)
    back = lax.all_to_all(starts, "sp", split_axis=0, concat_axis=0, tiled=True)
    late = chunk_reads(1, 2, *reads)
    return finish(back, early, late, norm_gain, columns)[None]


def solution(mesh):
    split_mesh = Mesh(mesh.devices.reshape(mesh.shape["sp"], 8, 2), ("sp", "dp_0", "dp_1"))
    placed = (
        P(DP, "sp", None),
        P(DP, "sp", None),
        P(DP, "sp", None),
        P(DP, "sp", None),
        P(DP, "sp", None),
        P(),
        P(),
        P(),
        P(),
        P(None, DP),
    )
    return jax.shard_map(
        per_device, mesh=split_mesh, in_specs=placed, out_specs=P(DP, "sp", None), check_vma=False
    )
```

```python
import jax
import jax.numpy as jnp
from jax import lax
from jax.experimental import pallas as pl
from jax.experimental.pallas import tpu as pltpu
from jax.sharding import Mesh
from jax.sharding import PartitionSpec as P

HEAD = 64
PAIR = 2 * HEAD
SMALL = 16
DP = ("dp_0", "dp_1")
GROUP = 16
TOGETHER = 8
ABREAST = 8
RUN = 8
READS = 4
BLOCKS = 4
FLOPS_PER_US = 500_000_000
F32 = jnp.float32
BF16 = jnp.bfloat16


def dot(left, right):
    return lax.dot_general(left, right, (((1,), (0,)), ((), ())), preferred_element_type=F32)


def dot_nt(left, right):
    return lax.dot_general(left, right, (((1,), (1,)), ((), ())), preferred_element_type=F32)


def split(value):
    high = value.astype(BF16)
    low = (value - high.astype(F32)).astype(BF16)
    return high, low


def lanes(*parts):
    return jnp.concatenate(parts, axis=1)


def rows(*parts):
    return jnp.concatenate(parts, axis=0)


def half_turn(value):
    return pltpu.roll(value, HEAD, 1)


def product(left, right):
    count = left[0].shape[0]
    both = dot(rows(*left), lanes(*right))
    return both[:count, :PAIR] + (both[:count, PAIR:] + both[count:, :PAIR])


def iota(shape, dim):
    return lax.broadcasted_iota(jnp.int32, shape, dim)


def same_head():
    return (iota((PAIR, PAIR), 0) // HEAD == iota((PAIR, PAIR), 1) // HEAD).astype(F32).astype(BF16)


def spread_kernel_table(table_ref, length):
    row = iota((length, length), 0)
    col = iota((length, length), 1)
    for s in range(SMALL):
        table_ref[:, s * length : (s + 1) * length] = (
            (row == (col // SMALL) * SMALL + s).astype(F32).astype(BF16)
        )


def inverses(matrices, table_ref, length):
    blocks = length // SMALL
    lane_block = iota((SMALL, length), 1) // SMALL
    packed = []
    for m in matrices:
        compact = jnp.zeros((SMALL, length), F32)
        for at in range(blocks):
            compact = jnp.where(lane_block == at, m[at * SMALL : (at + 1) * SMALL], compact)
        packed.append(compact)
    high, low = split(rows(*packed))
    tall = high.shape[0]
    left = rows(high, low)
    eye = (iota((SMALL, length), 1) % SMALL == iota((SMALL, length), 0)).astype(F32)
    solved = [eye for _ in matrices]
    for s in range(0, SMALL, 2):
        both = dot(left, table_ref[:, s * length : (s + 2) * length])
        both = both[:tall] + both[tall:]
        for step in range(2):
            if s + step + 1 == SMALL:
                break
            column = both[:, step * length : (step + 1) * length]
            solved = [
                x - column[i * SMALL : (i + 1) * SMALL] * x[s + step : s + step + 1] for i, x in enumerate(solved)
            ]
        if s % 4:
            yield None
    own = [(lane_block == at).astype(F32).astype(BF16) for at in range(blocks)]
    parts = [tuple(rows(*(p * o for o in own)) for p in split(x)) for x in solved]
    pieces = [split(m) for m in matrices]
    apart = iota((length, length), 0) ^ iota((length, length), 1)
    block = SMALL
    while block < length:
        spans = range(0, length, 2 * block)
        odd = lambda m: rows(*(m[at + block : at + 2 * block] for at in spans))
        here = odd(((apart >= block) & (apart < 2 * block)).astype(F32).astype(BF16))
        gap = jnp.zeros((block, length), BF16)
        wide = lambda m: rows(*(x for i in range(len(spans)) for x in (gap, m[i * block : (i + 1) * block])))
        put = lambda m, t: rows(
            *(
                x
                for i, at in enumerate(spans)
                for x in (m[at : at + block], m[at + block : at + 2 * block] - t[i * block : (i + 1) * block])
            )
        )
        yield None
        inner = [split(product((odd(h) * here, odd(l) * here), x)) for (h, l), x in zip(pieces, parts)]
        yield None
        taken = [
            split(product((odd(h), odd(l)), (wide(dh), wide(dl)))) for (h, l), (dh, dl) in zip(parts, inner)
        ]
        parts = [(put(h, th), put(l, tl)) for (h, l), (th, tl) in zip(parts, taken)]
        block *= 2
    yield parts


def paired_left(value, first):
    high, low = split(value)
    turned = half_turn(value - high.astype(F32)).astype(BF16)
    return lanes(jnp.where(first, high, turned), high), lanes(jnp.where(first, turned, high), high)


def paired_right(high, low):
    gap = jnp.zeros((HEAD, high.shape[1]), BF16)
    return (
        rows(high[:HEAD], high[:HEAD], low[:HEAD], gap),
        rows(high[HEAD:], high[HEAD:], gap, low[HEAD:]),
    )


def local_kernel(
    k_ref, v_ref, dl_ref, rl_ref, du_ref, ru_ref, base_ref, msg_ref, inner_ref, right_ref, scale_ref, centre_ref, table_ref
):
    length = k_ref.shape[0]

    @pl.when(pl.program_id(0) == 0)
    def _():
        spread_kernel_table(table_ref, length)

    row = iota((length, length), 0)
    col = iota((length, length), 1)
    strict = row > col
    lower = (row >= col).astype(F32).astype(BF16)
    lower_twice = lanes(lower, lower)
    ones = same_head()
    ones_twice = rows(ones, ones)
    squashed = jnp.tanh(dl_ref[...].astype(F32)).astype(BF16)
    first = iota((length, PAIR), 1) < HEAD
    second_half = iota((HEAD, PAIR), 1) >= HEAD
    diagonal = iota((HEAD, PAIR), 0) == iota((HEAD, PAIR), 1)

    def prepare(p):
        span = slice(p * PAIR, (p + 1) * PAIR)
        decay_pre = (base_ref[:, span] + dot(squashed, du_ref[:, span])).astype(BF16).astype(F32)
        rate_pre = dot(rl_ref[...], ru_ref[:, span]).astype(BF16).astype(F32)
        yield None
        log_decay = (-0.6065306597126334) / (1.0 + jnp.exp(-decay_pre))
        rate = 0.5 + 0.5 * jnp.tanh(0.5 * rate_pre)
        k = k_ref[:, span].astype(F32)
        v = v_ref[:, span]
        v_turned = half_turn(v.astype(F32)).astype(BF16)
        squares = dot(lanes(*split(k * k)), ones_twice)
        unit = k * lax.rsqrt(1.0 + squares)
        erase = unit * rate
        running = dot(lower_twice, rows(*split(log_decay)))
        yield None
        before = running - log_decay
        centre = running[length // 2 : length // 2 + 1]
        final = running[length - 1 :]
        back = jnp.exp(centre - running)
        centre_decay = jnp.exp(centre)
        scale_ref[:, span] = jnp.exp(running - centre)
        centre_ref[:, span] = centre_decay
        columns = rows(jnp.exp(final - centre), jnp.exp(final) - 1.0, jnp.zeros((6, PAIR), F32)).T
        rest_decay = columns[:, :1]
        keep = columns[:, 1:2]
        erase_from = unit * jnp.exp(before - centre)
        key_to = (k * back).T
        erase_to = (erase * back).T
        right = split(lanes(key_to, erase_to))
        right_ref[p, 0], right_ref[p, 1] = right
        key_end = split(key_to * rest_decay)
        erase_end = split(erase_to * rest_decay)
        erase_start = erase_from * centre_decay
        starts = (erase_start, half_turn(erase_start))
        sides = zip(paired_left(erase_from, first), paired_right(*right))
        yield None
        paired = [dot(left, side) for left, side in sides]
        yield None
        made = []
        for h, pairings in enumerate(paired):
            key_pairs = split(jnp.where(strict, pairings[:, :length], 0.0))
            half = slice(h * HEAD, (h + 1) * HEAD)
            value = v if h else v_turned
            applied = dot(
                rows(lanes(*key_pairs), lanes(key_end[0][half], key_end[1][half])), rows(value, value)
            )
            made.append(
                dict(
                    head=2 * p + h,
                    lower=jnp.where(strict, pairings[:, length:], 0.0),
                    sides=split(jnp.where(first, starts[h], applied[:length])),
                    gained=applied[length:],
                    erase_end=(erase_end[0][half], erase_end[1][half]),
                    keep=keep[half],
                )
            )
        yield made

    def solve(stage):
        for solved in inverses([s["lower"] for s in stage], table_ref, length):
            yield
        inners = [split(product(m, s["sides"])) for s, m in zip(stage, solved)]
        yield
        for s, inner in zip(stage, inners):
            head = s["head"]
            inner_ref[head, 0], inner_ref[head, 1] = inner
            ended = product(s["erase_end"], inner)
            gained = jnp.where(second_half, s["gained"], jnp.where(diagonal, s["keep"], 0.0))
            msg_ref[head] = (gained - ended).astype(BF16)

    pairs = k_ref.shape[1] // PAIR
    stage = []
    for start in range(0, pairs, TOGETHER):
        for made in zip(*(prepare(p) for p in range(start, min(start + TOGETHER, pairs)))):
            pass
        stage += [head for pair in made for head in pair]
    for _ in solve(stage):
        pass


def read_kernel(q_ref, v_ref, scale_ref, centre_ref, right_ref, inner_ref, out_ref):
    length = q_ref.shape[0]
    within = iota((length, length), 0) >= iota((length, length), 1)
    first = iota((length, PAIR), 1) < HEAD

    def read(p):
        span = slice(p * PAIR, (p + 1) * PAIR)
        v = v_ref[:, span]
        v_turned = half_turn(v.astype(F32)).astype(BF16)
        read_mid = q_ref[:, span].astype(F32) * scale_ref[:, span]
        read_start = read_mid * centre_ref[:, span]
        starts = (read_start, half_turn(read_start))
        sides = paired_right(right_ref[p, 0], right_ref[p, 1])
        paired = [dot(left, side) for left, side in zip(paired_left(read_mid, first), sides)]
        yield
        parts = []
        for h, pairings in enumerate(paired):
            read_keys = split(jnp.where(within, pairings[:, :length], 0.0))
            read_erase = split(jnp.where(within, pairings[:, length:], 0.0))
            value = v if h else v_turned
            applied = dot(lanes(*read_keys), rows(value, value))
            taken = product(read_erase, (inner_ref[2 * p + h, 0], inner_ref[2 * p + h, 1]))
            parts.append((applied, taken))
        yield
        for h, (applied, taken) in enumerate(parts):
            high, low = split(jnp.where(first, starts[h], applied) - taken)
            out_ref[2 * p + h, 0] = high
            out_ref[2 * p + h, 1] = low
        yield

    pairs = q_ref.shape[1] // PAIR
    for start in range(0, pairs, READS):
        for _ in zip(*(read(p) for p in range(start, min(start + READS, pairs)))):
            pass


def scan_kernel(msg_ref, start_ref):
    chunks = msg_ref.shape[0]
    runs = chunks // RUN
    half = HEAD // 2
    first = iota((PAIR, PAIR), 1) < HEAD
    eye = (iota((PAIR, PAIR), 0) + HEAD == iota((PAIR, PAIR), 1)).astype(F32).astype(BF16)
    nothing = jnp.zeros((PAIR, PAIR), BF16)
    begin = (iota((PAIR, PAIR), 0) == HEAD + (iota((PAIR, PAIR), 1) % HEAD)).astype(F32)

    def put(i, state):
        start_ref[i] = jnp.where(first[:half], state[:half], state[half:]).astype(BF16)

    held = [[begin if r else begin[:HEAD]] for r in range(runs)]
    parts = [[split(h[0])] for h in held]
    for j in range(RUN):
        for r in range(runs):
            if j + 1 == RUN and r + 1 == runs:
                continue
            high, low = parts[r][j]
            tall = high.shape[0]
            left = lanes(jnp.where(first[:tall], high, eye[:tall]), jnp.where(first[:tall], low, nothing[:tall]))
            here = msg_ref[r * RUN + j]
            here = rows(here, here)
            held[r].append(held[r][j] + dot_nt(left, lanes(here, here)))
            parts[r].append(split(held[r][j + 1]))
    for j in range(RUN):
        put(j, held[0][j])
    state = held[0][RUN]
    for r in range(1, runs):
        put(r * RUN, state)
        high, low = split(state)
        blank = nothing[:HEAD]
        left = lanes(jnp.where(first[:HEAD], high, low), jnp.where(first[:HEAD], high, blank))
        for j in range(RUN, 0, -1):
            if j == RUN and r + 1 == runs:
                continue
            high, low = (x[HEAD:] for x in parts[r][j])
            moved = held[r][j][:HEAD] + dot(left, rows(high, high, low, blank))
            if j == RUN:
                state = moved
            else:
                put(r * RUN + j, moved)


def finish_kernel(start_ref, read_ref, gain_ref, w_ref, out_ref, mix_ref, here_ref, done_ref):
    copies = [pltpu.make_async_copy(w_ref.at[k], here_ref.at[k], done_ref.at[k]) for k in range(w_ref.shape[0])]
    for copy in copies:
        copy.start()
    length, width = mix_ref.shape
    ones = same_head()
    ones_twice = rows(ones, ones)
    half = HEAD // 2
    first = iota((half, PAIR), 1) < HEAD
    row = iota((HEAD, PAIR), 0)
    col = iota((HEAD, PAIR), 1)
    eyes = [(row + h * HEAD == col).astype(F32) for h in range(2)]
    def mixed(p):
        span = slice(p * PAIR, (p + 1) * PAIR)
        one = start_ref[2 * p].astype(F32)
        two = start_ref[2 * p + 1].astype(F32)
        states = rows(
            jnp.where(first, one, 0.0),
            jnp.where(first, half_turn(one), 0.0),
            jnp.where(first, 0.0, half_turn(two)),
            jnp.where(first, 0.0, two),
        ).T
        right = rows(states[:HEAD], eyes[0], states[HEAD:], eyes[1]).astype(BF16)
        yield
        left = rows(*(lanes(read_ref[2 * p, part], read_ref[2 * p + 1, part]) for part in range(2)))
        readout = dot(left, right)
        yield
        readout = readout[:length] + readout[length:]
        average = dot(lanes(*split(readout)), ones_twice) * (1.0 / HEAD)
        yield
        centred = readout - average
        variance = dot(lanes(*split(centred * centred)), ones_twice) * (1.0 / HEAD)
        yield
        normed = centred * lax.rsqrt(variance + 1.0)
        mix_ref[:, span] = (normed * gain_ref[:, span]).astype(BF16)
        yield

    for start in range(0, width // PAIR, ABREAST):
        for _ in zip(*(mixed(p) for p in range(start, start + ABREAST))):
            pass
    mix = mix_ref[...]
    for k in range(0, w_ref.shape[0], BLOCKS):
        for copy in copies[k : k + BLOCKS]:
            copy.wait()
        right = lanes(*(here_ref[j] for j in range(k, k + BLOCKS)))
        out_ref[:, k * 128 : (k + BLOCKS) * 128] = dot(mix, right).astype(BF16)


def budget(mib, us):
    return dict(
        compiler_params=pltpu.CompilerParams(vmem_limit_bytes=mib << 20),
        cost_estimate=pl.CostEstimate(flops=int(us * FLOPS_PER_US), transcendentals=0, bytes_accessed=1 << 20),
    )


def local_chunk(k, v, dl, rl, du, ru, base):
    length, width = k.shape
    heads = width // HEAD
    step = GROUP * HEAD
    wide = pl.BlockSpec((length, step), lambda i: (0, i))
    low = pl.BlockSpec(dl.shape, lambda i: (0, 0))
    up = pl.BlockSpec((du.shape[0], step), lambda i: (0, i))
    line = pl.BlockSpec((1, step), lambda i: (0, i))
    return pl.pallas_call(
        local_kernel,
        grid=(width // step,),
        in_specs=[wide, wide, low, low, up, up, line],
        out_specs=[
            pl.BlockSpec((GROUP, HEAD, PAIR), lambda i: (i, 0, 0)),
            pl.BlockSpec((GROUP, 2, length, PAIR), lambda i: (i, 0, 0, 0)),
            pl.BlockSpec((GROUP // 2, 2, PAIR, 2 * length), lambda i: (i, 0, 0, 0)),
            wide,
            line,
        ],
        out_shape=[
            jax.ShapeDtypeStruct((heads, HEAD, PAIR), BF16),
            jax.ShapeDtypeStruct((heads, 2, length, PAIR), BF16),
            jax.ShapeDtypeStruct((heads // 2, 2, PAIR, 2 * length), BF16),
            jax.ShapeDtypeStruct((length, width), F32),
            jax.ShapeDtypeStruct((1, width), F32),
        ],
        scratch_shapes=[pltpu.VMEM((length, SMALL * length), BF16)],
        name="local_chunk",
        **budget(60, 25),
    )(k, v, dl, rl, du, ru, base.reshape(1, width))


def chunk_reads(q, v, scale, centre, right, inner):
    length, width = q.shape
    heads = width // HEAD
    count = GROUP // 2
    step = count * HEAD
    steps = heads // count
    at = lambda i: i
    wide = pl.BlockSpec((length, step), lambda i: (0, at(i)))
    per_head = lambda place: pl.BlockSpec((count, 2, length, PAIR), lambda i: (place(i), 0, 0, 0))
    return pl.pallas_call(
        read_kernel,
        grid=(steps,),
        in_specs=[
            wide,
            wide,
            wide,
            pl.BlockSpec((1, step), lambda i: (0, at(i))),
            pl.BlockSpec((count // 2, 2, PAIR, 2 * length), lambda i: (at(i), 0, 0, 0)),
            per_head(at),
        ],
        out_specs=per_head(lambda i: i),
        out_shape=jax.ShapeDtypeStruct((heads, 2, length, PAIR), BF16),
        name="chunk_reads",
        **budget(60, 8),
    )(q, v, scale, centre, right, inner)


def scan_chunks(msg):
    chunks = msg.shape[0]
    return pl.pallas_call(
        scan_kernel,
        out_shape=jax.ShapeDtypeStruct((chunks, HEAD // 2, PAIR), BF16),
        name="scan_chunks",
        **budget(4, 6),
    )(msg)


def finish(starts, reads, gain, weight):
    length = reads.shape[2]
    width = gain.shape[0]
    return pl.pallas_call(
        finish_kernel,
        in_specs=[pl.BlockSpec(memory_space=pltpu.VMEM)] * 3 + [pl.BlockSpec(memory_space=pltpu.HBM)],
        out_shape=jax.ShapeDtypeStruct((length, weight.shape[0] * weight.shape[2]), BF16),
        scratch_shapes=[
            pltpu.VMEM((length, width), BF16),
            pltpu.VMEM(weight.shape, BF16),
            pltpu.SemaphoreType.DMA((weight.shape[0],)),
        ],
        name="finish",
        **budget(60, 6),
    )(starts, reads, gain.reshape(1, width), weight)


def per_device(
    query_rows, key_rows, value_rows, decay_low, rate_low, decay_up, rate_up, decay_base, norm_gain, out_weight
):
    columns = lax.all_gather(out_weight, DP)
    msg, inner, right, scale, centre = local_chunk(
        key_rows[0], value_rows[0], decay_low[0], rate_low[0], decay_up, rate_up, decay_base
    )
    reads = (query_rows[0], value_rows[0], scale, centre, right, inner)
    here = lax.all_to_all(msg, "sp", split_axis=0, concat_axis=0, tiled=True)
    read = chunk_reads(*reads)
    here, read = lax.optimization_barrier((here, read))
    starts = scan_chunks(here)
    back = lax.all_to_all(starts, "sp", split_axis=0, concat_axis=0, tiled=True)
    return finish(back, read, norm_gain, columns)[None]


def solution(mesh):
    split_mesh = Mesh(mesh.devices.reshape(mesh.shape["sp"], 8, 2), ("sp", "dp_0", "dp_1"))
    placed = (
        P(DP, "sp", None),
        P(DP, "sp", None),
        P(DP, "sp", None),
        P(DP, "sp", None),
        P(DP, "sp", None),
        P(),
        P(),
        P(),
        P(),
        P(None, DP),
    )
    return jax.shard_map(
        per_device, mesh=split_mesh, in_specs=placed, out_specs=P(DP, "sp", None), check_vma=False
    )
```

```python
import jax
import jax.numpy as jnp
from jax import lax
from jax.experimental import pallas as pl
from jax.experimental.pallas import tpu as pltpu
from jax.sharding import Mesh
from jax.sharding import PartitionSpec as P

HEAD = 64
PAIR = 2 * HEAD
SMALL = 16
DP = ("dp_0", "dp_1")
GROUP = 16
TOGETHER = 8
ABREAST = 8
RUN = 8
READS = 4
BLOCKS = 4
FLOPS_PER_US = 500_000_000
F32 = jnp.float32
BF16 = jnp.bfloat16


def dot(left, right):
    return lax.dot_general(left, right, (((1,), (0,)), ((), ())), preferred_element_type=F32)


def dot_nt(left, right):
    return lax.dot_general(left, right, (((1,), (1,)), ((), ())), preferred_element_type=F32)


def split(value):
    high = value.astype(BF16)
    low = (value - high.astype(F32)).astype(BF16)
    return high, low


def lanes(*parts):
    return jnp.concatenate(parts, axis=1)


def rows(*parts):
    return jnp.concatenate(parts, axis=0)


def half_turn(value):
    return pltpu.roll(value, HEAD, 1)


def product(left, right):
    count = left[0].shape[0]
    both = dot(rows(*left), lanes(*right))
    return both[:count, :PAIR] + (both[:count, PAIR:] + both[count:, :PAIR])


def iota(shape, dim):
    return lax.broadcasted_iota(jnp.int32, shape, dim)


def same_head():
    return (iota((PAIR, PAIR), 0) // HEAD == iota((PAIR, PAIR), 1) // HEAD).astype(F32).astype(BF16)


def spread_kernel_table(table_ref, length):
    row = iota((length, length), 0)
    col = iota((length, length), 1)
    for s in range(SMALL):
        table_ref[:, s * length : (s + 1) * length] = (
            (row == (col // SMALL) * SMALL + s).astype(F32).astype(BF16)
        )


def inverses(matrices, table_ref, length):
    blocks = length // SMALL
    lane_block = iota((SMALL, length), 1) // SMALL
    packed = []
    for m in matrices:
        compact = jnp.zeros((SMALL, length), F32)
        for at in range(blocks):
            compact = jnp.where(lane_block == at, m[at * SMALL : (at + 1) * SMALL], compact)
        packed.append(compact)
    high, low = split(rows(*packed))
    tall = high.shape[0]
    left = rows(high, low)
    eye = (iota((SMALL, length), 1) % SMALL == iota((SMALL, length), 0)).astype(F32)
    solved = [eye for _ in matrices]
    for s in range(0, SMALL, 2):
        both = dot(left, table_ref[:, s * length : (s + 2) * length])
        both = both[:tall] + both[tall:]
        for step in range(2):
            if s + step + 1 == SMALL:
                break
            column = both[:, step * length : (step + 1) * length]
            solved = [
                x - column[i * SMALL : (i + 1) * SMALL] * x[s + step : s + step + 1] for i, x in enumerate(solved)
            ]
        if s % 4:
            yield None
    own = [(lane_block == at).astype(F32).astype(BF16) for at in range(blocks)]
    parts = [tuple(rows(*(p * o for o in own)) for p in split(x)) for x in solved]
    pieces = [split(m) for m in matrices]
    apart = iota((length, length), 0) ^ iota((length, length), 1)
    block = SMALL
    while block < length:
        spans = range(0, length, 2 * block)
        odd = lambda m: rows(*(m[at + block : at + 2 * block] for at in spans))
        here = odd(((apart >= block) & (apart < 2 * block)).astype(F32).astype(BF16))
        gap = jnp.zeros((block, length), BF16)
        wide = lambda m: rows(*(x for i in range(len(spans)) for x in (gap, m[i * block : (i + 1) * block])))
        put = lambda m, t: rows(
            *(
                x
                for i, at in enumerate(spans)
                for x in (m[at : at + block], m[at + block : at + 2 * block] - t[i * block : (i + 1) * block])
            )
        )
        yield None
        inner = [split(product((odd(h) * here, odd(l) * here), x)) for (h, l), x in zip(pieces, parts)]
        yield None
        taken = [
            split(product((odd(h), odd(l)), (wide(dh), wide(dl)))) for (h, l), (dh, dl) in zip(parts, inner)
        ]
        parts = [(put(h, th), put(l, tl)) for (h, l), (th, tl) in zip(parts, taken)]
        block *= 2
    yield parts


def paired_left(value, first):
    high, low = split(value)
    turned = half_turn(value - high.astype(F32)).astype(BF16)
    return lanes(jnp.where(first, high, turned), high), lanes(jnp.where(first, turned, high), high)


def paired_right(high, low):
    gap = jnp.zeros((HEAD, high.shape[1]), BF16)
    return (
        rows(high[:HEAD], high[:HEAD], low[:HEAD], gap),
        rows(high[HEAD:], high[HEAD:], gap, low[HEAD:]),
    )


def local_kernel(
    k_ref, v_ref, dl_ref, rl_ref, du_ref, ru_ref, base_ref, msg_ref, inner_ref, right_ref, scale_ref, centre_ref, table_ref
):
    length = k_ref.shape[0]

    @pl.when(pl.program_id(0) == 0)
    def _():
        spread_kernel_table(table_ref, length)

    row = iota((length, length), 0)
    col = iota((length, length), 1)
    strict = row > col
    lower = (row >= col).astype(F32).astype(BF16)
    lower_twice = lanes(lower, lower)
    ones = same_head()
    ones_twice = rows(ones, ones)
    squashed = jnp.tanh(dl_ref[...].astype(F32)).astype(BF16)
    first = iota((length, PAIR), 1) < HEAD
    second_half = iota((HEAD, PAIR), 1) >= HEAD
    diagonal = iota((HEAD, PAIR), 0) == iota((HEAD, PAIR), 1)

    def prepare(p):
        span = slice(p * PAIR, (p + 1) * PAIR)
        decay_pre = (base_ref[:, span] + dot(squashed, du_ref[:, span])).astype(BF16).astype(F32)
        rate_pre = dot(rl_ref[...], ru_ref[:, span]).astype(BF16).astype(F32)
        yield None
        log_decay = (-0.6065306597126334) / (1.0 + jnp.exp(-decay_pre))
        rate = 0.5 + 0.5 * jnp.tanh(0.5 * rate_pre)
        k = k_ref[:, span].astype(F32)
        v = v_ref[:, span]
        v_turned = half_turn(v.astype(F32)).astype(BF16)
        squares = dot(lanes(*split(k * k)), ones_twice)
        unit = k * lax.rsqrt(1.0 + squares)
        erase = unit * rate
        running = dot(lower_twice, rows(*split(log_decay)))
        yield None
        before = running - log_decay
        centre = running[length // 2 : length // 2 + 1]
        final = running[length - 1 :]
        back = jnp.exp(centre - running)
        centre_decay = jnp.exp(centre)
        scale_ref[:, span] = jnp.exp(running - centre)
        centre_ref[:, span] = centre_decay
        columns = rows(jnp.exp(final - centre), jnp.exp(final) - 1.0, jnp.zeros((6, PAIR), F32)).T
        rest_decay = columns[:, :1]
        keep = columns[:, 1:2]
        erase_from = unit * jnp.exp(before - centre)
        key_to = (k * back).T
        erase_to = (erase * back).T
        right = split(lanes(key_to, erase_to))
        right_ref[p, 0], right_ref[p, 1] = right
        key_end = split(key_to * rest_decay)
        erase_end = split(erase_to * rest_decay)
        erase_start = erase_from * centre_decay
        starts = (erase_start, half_turn(erase_start))
        sides = zip(paired_left(erase_from, first), paired_right(*right))
        yield None
        paired = [dot(left, side) for left, side in sides]
        yield None
        made = []
        for h, pairings in enumerate(paired):
            key_pairs = split(jnp.where(strict, pairings[:, :length], 0.0))
            half = slice(h * HEAD, (h + 1) * HEAD)
            value = v if h else v_turned
            applied = dot(
                rows(lanes(*key_pairs), lanes(key_end[0][half], key_end[1][half])), rows(value, value)
            )
            made.append(
                dict(
                    head=2 * p + h,
                    lower=jnp.where(strict, pairings[:, length:], 0.0),
                    sides=split(jnp.where(first, starts[h], applied[:length])),
                    gained=applied[length:],
                    erase_end=(erase_end[0][half], erase_end[1][half]),
                    keep=keep[half],
                )
            )
        yield made

    def solve(stage):
        for solved in inverses([s["lower"] for s in stage], table_ref, length):
            yield
        inners = [split(product(m, s["sides"])) for s, m in zip(stage, solved)]
        yield
        for s, inner in zip(stage, inners):
            head = s["head"]
            inner_ref[head, 0], inner_ref[head, 1] = inner
            ended = product(s["erase_end"], inner)
            gained = jnp.where(second_half, s["gained"], jnp.where(diagonal, s["keep"], 0.0))
            msg_ref[head] = (gained - ended).astype(BF16)

    pairs = k_ref.shape[1] // PAIR
    stage = []
    for start in range(0, pairs, TOGETHER):
        for made in zip(*(prepare(p) for p in range(start, min(start + TOGETHER, pairs)))):
            pass
        stage += [head for pair in made for head in pair]
    for _ in solve(stage):
        pass


def read_kernel(q_ref, v_ref, scale_ref, centre_ref, right_ref, inner_ref, out_ref):
    length = q_ref.shape[0]
    within = iota((length, length), 0) >= iota((length, length), 1)
    first = iota((length, PAIR), 1) < HEAD

    def read(p):
        span = slice(p * PAIR, (p + 1) * PAIR)
        v = v_ref[:, span]
        v_turned = half_turn(v.astype(F32)).astype(BF16)
        read_mid = q_ref[:, span].astype(F32) * scale_ref[:, span]
        read_start = read_mid * centre_ref[:, span]
        starts = (read_start, half_turn(read_start))
        sides = paired_right(right_ref[p, 0], right_ref[p, 1])
        paired = [dot(left, side) for left, side in zip(paired_left(read_mid, first), sides)]
        yield
        parts = []
        for h, pairings in enumerate(paired):
            read_keys = split(jnp.where(within, pairings[:, :length], 0.0))
            read_erase = split(jnp.where(within, pairings[:, length:], 0.0))
            value = v if h else v_turned
            applied = dot(lanes(*read_keys), rows(value, value))
            taken = product(read_erase, (inner_ref[2 * p + h, 0], inner_ref[2 * p + h, 1]))
            parts.append((applied, taken))
        yield
        for h, (applied, taken) in enumerate(parts):
            high, low = split(jnp.where(first, starts[h], applied) - taken)
            out_ref[2 * p + h, 0] = high
            out_ref[2 * p + h, 1] = low
        yield

    pairs = q_ref.shape[1] // PAIR
    for start in range(0, pairs, READS):
        for _ in zip(*(read(p) for p in range(start, min(start + READS, pairs)))):
            pass


def scan_kernel(msg_ref, start_ref):
    chunks = msg_ref.shape[0]
    runs = chunks // RUN
    half = HEAD // 2
    first = iota((PAIR, PAIR), 1) < HEAD
    eye = (iota((PAIR, PAIR), 0) + HEAD == iota((PAIR, PAIR), 1)).astype(F32).astype(BF16)
    nothing = jnp.zeros((PAIR, PAIR), BF16)
    begin = (iota((PAIR, PAIR), 0) == HEAD + (iota((PAIR, PAIR), 1) % HEAD)).astype(F32)

    def put(i, state):
        start_ref[i] = jnp.where(first[:half], state[:half], state[half:]).astype(BF16)

    held = [[begin if r else begin[:HEAD]] for r in range(runs)]
    parts = [[split(h[0])] for h in held]
    for j in range(RUN):
        for r in range(runs):
            if j + 1 == RUN and r + 1 == runs:
                continue
            high, low = parts[r][j]
            tall = high.shape[0]
            left = lanes(jnp.where(first[:tall], high, eye[:tall]), jnp.where(first[:tall], low, nothing[:tall]))
            here = msg_ref[r * RUN + j]
            here = rows(here, here)
            held[r].append(held[r][j] + dot_nt(left, lanes(here, here)))
            parts[r].append(split(held[r][j + 1]))
    for j in range(RUN):
        put(j, held[0][j])
    state = held[0][RUN]
    for r in range(1, runs):
        put(r * RUN, state)
        high, low = split(state)
        blank = nothing[:HEAD]
        left = lanes(jnp.where(first[:HEAD], high, low), jnp.where(first[:HEAD], high, blank))
        for j in range(RUN, 0, -1):
            if j == RUN and r + 1 == runs:
                continue
            high, low = (x[HEAD:] for x in parts[r][j])
            moved = held[r][j][:HEAD] + dot(left, rows(high, high, low, blank))
            if j == RUN:
                state = moved
            else:
                put(r * RUN + j, moved)


def finish_kernel(start_ref, read_ref, gain_ref, w_ref, out_ref, mix_ref, here_ref, done_ref):
    copies = [pltpu.make_async_copy(w_ref.at[k], here_ref.at[k], done_ref.at[k]) for k in range(w_ref.shape[0])]
    for copy in copies:
        copy.start()
    length, width = mix_ref.shape
    ones = same_head()
    ones_twice = rows(ones, ones)
    half = HEAD // 2
    first = iota((half, PAIR), 1) < HEAD
    row = iota((HEAD, PAIR), 0)
    col = iota((HEAD, PAIR), 1)
    eyes = [(row + h * HEAD == col).astype(F32) for h in range(2)]
    def mixed(p):
        span = slice(p * PAIR, (p + 1) * PAIR)
        one = start_ref[2 * p].astype(F32)
        two = start_ref[2 * p + 1].astype(F32)
        states = rows(
            jnp.where(first, one, 0.0),
            jnp.where(first, half_turn(one), 0.0),
            jnp.where(first, 0.0, half_turn(two)),
            jnp.where(first, 0.0, two),
        ).T
        right = rows(states[:HEAD], eyes[0], states[HEAD:], eyes[1]).astype(BF16)
        yield
        left = rows(*(lanes(read_ref[2 * p, part], read_ref[2 * p + 1, part]) for part in range(2)))
        readout = dot(left, right)
        yield
        readout = readout[:length] + readout[length:]
        average = dot(lanes(*split(readout)), ones_twice) * (1.0 / HEAD)
        yield
        centred = readout - average
        variance = dot(lanes(*split(centred * centred)), ones_twice) * (1.0 / HEAD)
        yield
        normed = centred * lax.rsqrt(variance + 1.0)
        mix_ref[:, span] = (normed * gain_ref[:, span]).astype(BF16)
        yield

    for start in range(0, width // PAIR, ABREAST):
        for _ in zip(*(mixed(p) for p in range(start, start + ABREAST))):
            pass
    mix = mix_ref[...]
    for k in range(0, w_ref.shape[0], BLOCKS):
        for copy in copies[k : k + BLOCKS]:
            copy.wait()
        right = lanes(*(here_ref[j] for j in range(k, k + BLOCKS)))
        out_ref[:, k * 128 : (k + BLOCKS) * 128] = dot(mix, right).astype(BF16)


def budget(mib, us):
    return dict(
        compiler_params=pltpu.CompilerParams(vmem_limit_bytes=mib << 20),
        cost_estimate=pl.CostEstimate(flops=int(us * FLOPS_PER_US), transcendentals=0, bytes_accessed=1 << 20),
    )


def local_chunk(k, v, dl, rl, du, ru, base):
    length, width = k.shape
    heads = width // HEAD
    step = GROUP * HEAD
    wide = pl.BlockSpec((length, step), lambda i: (0, i))
    low = pl.BlockSpec(dl.shape, lambda i: (0, 0))
    up = pl.BlockSpec((du.shape[0], step), lambda i: (0, i))
    line = pl.BlockSpec((1, step), lambda i: (0, i))
    return pl.pallas_call(
        local_kernel,
        grid=(width // step,),
        in_specs=[wide, wide, low, low, up, up, line],
        out_specs=[
            pl.BlockSpec((GROUP, HEAD, PAIR), lambda i: (i, 0, 0)),
            pl.BlockSpec((GROUP, 2, length, PAIR), lambda i: (i, 0, 0, 0)),
            pl.BlockSpec((GROUP // 2, 2, PAIR, 2 * length), lambda i: (i, 0, 0, 0)),
            wide,
            line,
        ],
        out_shape=[
            jax.ShapeDtypeStruct((heads, HEAD, PAIR), BF16),
            jax.ShapeDtypeStruct((heads, 2, length, PAIR), BF16),
            jax.ShapeDtypeStruct((heads // 2, 2, PAIR, 2 * length), BF16),
            jax.ShapeDtypeStruct((length, width), F32),
            jax.ShapeDtypeStruct((1, width), F32),
        ],
        scratch_shapes=[pltpu.VMEM((length, SMALL * length), BF16)],
        name="local_chunk",
        **budget(60, 25),
    )(k, v, dl, rl, du, ru, base.reshape(1, width))


def chunk_reads(q, v, scale, centre, right, inner):
    length, width = q.shape
    heads = width // HEAD
    count = GROUP // 2
    step = count * HEAD
    steps = heads // count
    at = lambda i: i
    wide = pl.BlockSpec((length, step), lambda i: (0, at(i)))
    per_head = lambda place: pl.BlockSpec((count, 2, length, PAIR), lambda i: (place(i), 0, 0, 0))
    return pl.pallas_call(
        read_kernel,
        grid=(steps,),
        in_specs=[
            wide,
            wide,
            wide,
            pl.BlockSpec((1, step), lambda i: (0, at(i))),
            pl.BlockSpec((count // 2, 2, PAIR, 2 * length), lambda i: (at(i), 0, 0, 0)),
            per_head(at),
        ],
        out_specs=per_head(lambda i: i),
        out_shape=jax.ShapeDtypeStruct((heads, 2, length, PAIR), BF16),
        name="chunk_reads",
        **budget(60, 8),
    )(q, v, scale, centre, right, inner)


def scan_chunks(msg):
    chunks = msg.shape[0]
    return pl.pallas_call(
        scan_kernel,
        out_shape=jax.ShapeDtypeStruct((chunks, HEAD // 2, PAIR), BF16),
        name="scan_chunks",
        **budget(4, 6),
    )(msg)


def finish(starts, reads, gain, weight):
    length = reads.shape[2]
    width = gain.shape[0]
    return pl.pallas_call(
        finish_kernel,
        in_specs=[pl.BlockSpec(memory_space=pltpu.VMEM)] * 3 + [pl.BlockSpec(memory_space=pltpu.HBM)],
        out_shape=jax.ShapeDtypeStruct((length, weight.shape[0] * weight.shape[2]), BF16),
        scratch_shapes=[
            pltpu.VMEM((length, width), BF16),
            pltpu.VMEM(weight.shape, BF16),
            pltpu.SemaphoreType.DMA((weight.shape[0],)),
        ],
        name="finish",
        **budget(52, 6),
    )(starts, reads, gain.reshape(1, width), weight)


def per_device(
    query_rows, key_rows, value_rows, decay_low, rate_low, decay_up, rate_up, decay_base, norm_gain, out_weight
):
    columns = lax.all_gather(out_weight, DP)
    msg, inner, right, scale, centre = local_chunk(
        key_rows[0], value_rows[0], decay_low[0], rate_low[0], decay_up, rate_up, decay_base
    )
    reads = (query_rows[0], value_rows[0], scale, centre, right, inner)
    here = lax.all_to_all(msg, "sp", split_axis=0, concat_axis=0, tiled=True)
    read = chunk_reads(*reads)
    here, read = lax.optimization_barrier((here, read))
    starts = scan_chunks(here)
    back = lax.all_to_all(starts, "sp", split_axis=0, concat_axis=0, tiled=True)
    return finish(back, read, norm_gain, columns)[None]


def solution(mesh):
    split_mesh = Mesh(mesh.devices.reshape(mesh.shape["sp"], 8, 2), ("sp", "dp_0", "dp_1"))
    placed = (
        P(DP, "sp", None),
        P(DP, "sp", None),
        P(DP, "sp", None),
        P(DP, "sp", None),
        P(DP, "sp", None),
        P(),
        P(),
        P(),
        P(),
        P(None, DP),
    )
    return jax.shard_map(
        per_device, mesh=split_mesh, in_specs=placed, out_specs=P(DP, "sp", None), check_vma=False
    )
```
